128 devices in a mesh: sp: 32 (over z, y, core), tp: 4 (over x).
Axes of the slice: x: 4, y: 4, z: 4, core: 2. Of those that a mesh axis runs over, the one named last changes fastest.
Arguments:
- hidden: bfloat16 [8192, 4096], P('sp'), as said below
- key_weight: bfloat16 [4096, 1024], P(None, 'tp'), as said below
- queries: bfloat16 [8192, 4096], P('sp', 'tp'), as said below
- values: bfloat16 [8192, 1024], P('sp', 'tp'), as said below
- map_out: bfloat16 [8192, 8192], P('sp', 'tp'), as said below
- log_sums: float32 [32, 8192], P('tp', 'sp'), as said below
- out_grad: bfloat16 [8192, 4096], P('sp', 'tp'), may hold values from -6 to 6
- mixing: float32 [16], P('tp'), may hold values from 0.3 to 0.8
- out_gain: float32 [256], replicated, may hold values from 0.1 to 1.9
Outputs:
- grad_query: bfloat16 [8192, 4096], P('sp', 'tp')
- grad_key: bfloat16 [8192, 1024], P('sp', 'tp')
- grad_value: bfloat16 [8192, 1024], P('sp', 'tp')
- grad_weight: float32 [4096, 1024], P('sp', 'tp')
The draws below stay inside these ranges and needn't reach their ends.
Inputs may be any that keep to these rules, and one draw needn't show every extreme that they name: `hidden`: inputs of order one. `key_weight`: entries of order 1 / sqrt(4096) times a constant. `queries`: entries of order one. `values`: entries of order one. `log_sums`: for head h, map m and row i: the logarithm of the sum over keys j <= i of exp(scores[h, m](i, j)), with key_rows formed as in the reference program. `map_out`: for head h and map m: the row's weights exp(scores - log_sums) over keys j <= i times the values of key head g(h), rounded to bfloat16.
All inputs are finite; a program needn't handle non-finite values.
Results may differ from the reference program's by a relative error of at most 0.02.
Values may be sent and summed in bfloat16 or wider, within the bound.
A program may use at most 256 MiB of HBM per device.

```python
import math
import jax
import jax.numpy as jnp
from jax import lax

D = 4096
HEADS = 16
KV_HEADS = 4
HEAD_DIM = 128
V_DIM = 256
TOKENS = 8192


def base_arrays(key):
    key_hidden = jax.random.fold_in(key, 101)
    key_weight = jax.random.fold_in(key, 102)
    key_query = jax.random.fold_in(key, 103)
    key_value = jax.random.fold_in(key, 104)
    hidden = jax.random.normal(key_hidden, (TOKENS, D), jnp.float32)
    queries = jax.random.normal(key_query, (TOKENS, HEADS * 2 * HEAD_DIM), jnp.float32)
    weight = jax.random.normal(key_weight, (D, KV_HEADS * 2 * HEAD_DIM), jnp.float32) * (1.5 / math.sqrt(D))
    values = jax.random.normal(key_value, (TOKENS, KV_HEADS * V_DIM), jnp.float32)
    return (hidden.astype(jnp.bfloat16), weight.astype(jnp.bfloat16), queries.astype(jnp.bfloat16), values.astype(jnp.bfloat16))


def forward_arrays(key):
    hidden, weight, queries, values = base_arrays(key)
    key_rows = jnp.dot(hidden, weight, preferred_element_type=jnp.float32).astype(jnp.bfloat16).astype(jnp.float32)
    per_group = HEADS // KV_HEADS
    block_rows = 128 if TOKENS % 128 == 0 else TOKENS
    n_blocks = TOKENS // block_rows
    query_all = queries.astype(jnp.float32).reshape(n_blocks, block_rows, KV_HEADS, per_group, 2, HEAD_DIM)
    key_all = key_rows.reshape(TOKENS, KV_HEADS, 2, HEAD_DIM)
    value_all = values.astype(jnp.float32).reshape(TOKENS, KV_HEADS, V_DIM)
    positions = jnp.arange(TOKENS, dtype=jnp.int32).reshape(n_blocks, block_rows)
    key_pos = jnp.arange(TOKENS, dtype=jnp.int32)
    sums_list, outs_list = ([], [])
    for head_group in range(KV_HEADS):
        key_g = key_all[:, head_group]
        value_g = value_all[:, head_group]

        def one_block(inputs):
            query_block, query_pos = inputs
            scores = jnp.einsum('bpmd,tmd->pmbt', query_block[:, head_group], key_g) * HEAD_DIM ** (-0.5)
            visible = key_pos[None, :] <= query_pos[:, None]
            scores = jnp.where(visible, scores, -1e+30)
            row_max = jnp.max(scores, axis=-1, keepdims=True)
            log_sum = row_max + jnp.log(jnp.sum(jnp.exp(scores - row_max), axis=-1, keepdims=True))
            probs_map = jnp.exp(scores - log_sum)
            outputs = jnp.einsum('pmbt,tv->bpmv', probs_map, value_g)
            return (log_sum[..., 0], outputs)
        sums_g, outs_g = lax.map(one_block, (query_all, positions))
        sums_list.append(jnp.transpose(sums_g, (1, 2, 0, 3)).reshape(per_group * 2, TOKENS))
        outs_list.append(outs_g.reshape(TOKENS, per_group * 2 * V_DIM))
    return (jnp.concatenate(sums_list, axis=0), jnp.concatenate(outs_list, axis=1).astype(jnp.bfloat16))


def draw_hidden(key, part):
    return base_arrays(key)[0]


def draw_key_weight(key, part):
    return base_arrays(key)[1]


def draw_queries(key, part):
    return base_arrays(key)[2]


def draw_values(key, part):
    return base_arrays(key)[3]


def draw_log_sums(key, part):
    return forward_arrays(key)[0]


def draw_map_out(key, part):
    return forward_arrays(key)[1]


def spiked(entries, stream_key, source, target, blocks, factor):
    def block_of(axis_at):
        return (jnp.arange(entries.shape[axis_at]) // (entries.shape[axis_at] // blocks)).reshape((-1,) + (1,) * (entries.ndim - 1 - axis_at))

    first = jax.random.permutation(stream_key, blocks)[block_of(target)]
    second = (block_of(target) + blocks // 2) % blocks
    return jnp.where((block_of(source) == first) | (block_of(source) == second), factor * entries, entries)


def steps_of(stream_key, shape, cuts, smallest, high):
    def one(dim, blocks):
        heights = jax.random.uniform(jax.random.fold_in(jax.random.fold_in(stream_key, 6), dim), (blocks,), jnp.float32, smallest / len(cuts), high / len(cuts))
        return jnp.repeat(jnp.exp(heights), shape[dim] // blocks).reshape((-1,) + (1,) * (len(shape) - dim - 1))

    level = one(*cuts[0])
    for cut in cuts[1:]:
        level = level * one(*cut)
    return level


def bell_draw_with(own_key, extent, deviation, most, cuts, heavy, held_as=jnp.bfloat16):
    entries = deviation * jax.random.normal(own_key, extent, jnp.float32)
    if cuts:
        entries = entries * steps_of(own_key, extent, cuts, -0.22, 0.18)
    return jnp.clip(spiked(entries, jax.random.fold_in(own_key, 3), *heavy), -most, most).astype(held_as)


def setup_inputs(seed: int = 0) -> dict:
    seeds = jax.random.split(jax.random.key(seed), 10)
    hidden = draw_hidden(jax.random.fold_in(seeds[9], 71), 0)
    key_weight = draw_key_weight(jax.random.fold_in(seeds[9], 71), 0)
    queries = draw_queries(jax.random.fold_in(seeds[9], 71), 0)
    values = draw_values(jax.random.fold_in(seeds[9], 71), 0)
    map_out = draw_map_out(jax.random.fold_in(seeds[9], 71), 0)
    log_sums = draw_log_sums(jax.random.fold_in(seeds[9], 71), 0)
    out_grad = bell_draw_with(seeds[6], (TOKENS, HEADS * V_DIM), 1.0, 6.0, ((0, 32), (1, 4)), (0, 1, 32, 2.75))
    mixing = jnp.clip(0.3 + 0.5 * jax.random.uniform(seeds[7], (HEADS,), jnp.float32) ** steps_of(seeds[7], (HEADS,), ((0, 4),), -0.2, 0.2), 0.3, 0.8)
    out_gain = jnp.clip(1.0 + 0.18 * jax.random.normal(seeds[8], (V_DIM,), jnp.float32), 0.1, 1.9)
    return {"hidden": hidden, "key_weight": key_weight, "queries": queries, "values": values, "map_out": map_out, "log_sums": log_sums, "out_grad": out_grad, "mixing": mixing, "out_gain": out_gain}


OUT_SCALE = 0.8
NORM_EPS = 1e-06

def head_terms(out_grad, map_out, mixing, out_gain):
    rows_here = out_grad.shape[0]
    heads_here = mixing.shape[0]
    v_width = out_gain.shape[0]
    maps_out = map_out.astype(jnp.float32).reshape(rows_here, heads_here, 2, v_width)
    pre_norm = maps_out[:, :, 0] - mixing[None, :, None] * maps_out[:, :, 1]
    inverse = lax.rsqrt(lax.optimization_barrier(jnp.mean(pre_norm * pre_norm, axis=-1, keepdims=True)) + NORM_EPS)
    upstream = out_grad.astype(jnp.float32).reshape(rows_here, heads_here, v_width) * out_gain * OUT_SCALE
    d_out = inverse * (upstream - pre_norm * inverse * inverse * lax.optimization_barrier(jnp.mean(upstream * pre_norm, axis=-1, keepdims=True)))
    row_terms = lax.optimization_barrier(jnp.sum(d_out[:, :, None, :] * maps_out, axis=-1)).reshape(rows_here, heads_here * 2)
    return (d_out.reshape(rows_here, heads_here * v_width).astype(jnp.bfloat16), row_terms)

def round_trip(array):
    return lax.optimization_barrier(array.astype(jnp.bfloat16)).astype(jnp.float32)

def block_grads(query_blk, d_blk, log_blk, term_blk, query_pos, key_all, value_all, key_pos, mix_blk):
    scale = query_blk.shape[-1] ** (-0.5)
    log_part = jnp.transpose(log_blk, (1, 2, 3, 0))[..., None]
    term_part = jnp.transpose(term_blk, (1, 2, 3, 0))[..., None]
    scores = jnp.einsum('rgpmd,kgmd->gpmrk', query_blk, key_all) * scale
    visible = key_pos[None, :] <= query_pos[:, None]
    probs_map = jnp.exp(jnp.where(visible, scores - log_part, -1e+30))
    d_attn = jnp.einsum('rgpv,kgv->gprk', d_blk, value_all)
    mix_cols = mix_blk[:, :, None, None]
    weights_a = round_trip(probs_map[:, :, 0] - mix_cols * probs_map[:, :, 1])
    d_scores = round_trip(jnp.stack([probs_map[:, :, 0] * (d_attn - term_part[:, :, 0]), -mix_cols * probs_map[:, :, 1] * (d_attn - term_part[:, :, 1])], axis=2))
    grad_q = jnp.einsum('gpmrk,kgmd->rgpmd', d_scores, key_all) * scale
    grad_k = jnp.einsum('gpmrk,rgpmd->kgmd', d_scores, query_blk) * scale
    grad_v = jnp.einsum('gprk,rgpv->kgv', weights_a, d_blk)
    return (grad_q, grad_k, grad_v)

def reference(hidden, key_weight, queries, values, map_out, log_sums, out_grad, mixing, out_gain):
    total = queries.shape[0]
    per_group = HEADS // KV_HEADS
    key_rows = jnp.dot(hidden, key_weight, preferred_element_type=jnp.float32).astype(jnp.bfloat16)
    d_rows, row_terms = head_terms(out_grad, map_out, mixing, out_gain)
    query_all = queries.astype(jnp.float32).reshape(total, KV_HEADS, per_group, 2, HEAD_DIM)
    key_all = key_rows.astype(jnp.float32).reshape(total, KV_HEADS, 2, HEAD_DIM)
    value_all = values.astype(jnp.float32).reshape(total, KV_HEADS, V_DIM)
    d_all = d_rows.astype(jnp.float32).reshape(total, KV_HEADS, per_group, V_DIM)
    log_all = log_sums.T.reshape(total, KV_HEADS, per_group, 2)
    term_all = row_terms.reshape(total, KV_HEADS, per_group, 2)
    mix_all = mixing.reshape(KV_HEADS, per_group)
    block_rows = 256 if total % 256 == 0 else total
    n_blocks = total // block_rows
    key_pos = jnp.arange(total, dtype=jnp.int32)
    query_list, key_list, value_list = ([], [], [])
    for head_group in range(KV_HEADS):
        query_g = query_all[:, head_group:head_group + 1]
        d_g = d_all[:, head_group:head_group + 1]
        log_g = log_all[:, head_group:head_group + 1]
        term_g = term_all[:, head_group:head_group + 1]
        key_g = key_all[:, head_group:head_group + 1]
        value_g = value_all[:, head_group:head_group + 1]
        mix_g = mix_all[head_group:head_group + 1]

        def step_fn(carry, index):
            acc_key, acc_value = carry
            start = (index * block_rows).astype(jnp.int32)
            query_pos = start + jnp.arange(block_rows, dtype=jnp.int32)
            grad_q, grad_k, grad_v = block_grads(lax.dynamic_slice_in_dim(query_g, start, block_rows, 0), lax.dynamic_slice_in_dim(d_g, start, block_rows, 0), lax.dynamic_slice_in_dim(log_g, start, block_rows, 0), lax.dynamic_slice_in_dim(term_g, start, block_rows, 0), query_pos, key_g, value_g, key_pos, mix_g)
            return ((acc_key + grad_k, acc_value + grad_v), grad_q)
        init = (jnp.zeros((total, 1, 2, HEAD_DIM), jnp.float32), jnp.zeros((total, 1, V_DIM), jnp.float32))
        (acc_key, acc_value), grads_q = lax.scan(step_fn, init, jnp.arange(n_blocks, dtype=jnp.int32))
        query_list.append(grads_q.reshape(total, per_group * 2 * HEAD_DIM))
        key_list.append(acc_key.reshape(total, 2 * HEAD_DIM))
        value_list.append(acc_value.reshape(total, V_DIM))
    grad_query = jnp.concatenate(query_list, axis=1).astype(jnp.bfloat16)
    grad_key = jnp.concatenate(key_list, axis=1).astype(jnp.bfloat16)
    grad_value = jnp.concatenate(value_list, axis=1).astype(jnp.bfloat16)
    grad_weight = lax.dot_general(hidden, grad_key, (((0,), (0,)), ((), ())), preferred_element_type=jnp.float32)
    return (grad_query, grad_key, grad_value, grad_weight)
```

```python
import functools
import math

import jax
import jax.numpy as jnp
from jax import lax
from jax.experimental import pallas as pl
from jax.experimental.pallas import tpu as pltpu
from jax.sharding import PartitionSpec as P

HEAD_DIM = 128
V_DIM = 256
OUT_SCALE = 0.8
NORM_EPS = 1e-06
LOG2E = math.log2(math.e)
MESH_ID = pl.DeviceIdType.MESH
BF16 = jnp.bfloat16
F32 = jnp.float32


def nn(a, b):
    return jnp.dot(a, b, preferred_element_type=F32)


def kernel(n, heads, mix_ref, hid_hbm, kw_hbm, q_hbm, val_hbm, map_hbm, log_hbm, og_hbm, gain_hbm,
           gq_ref, gk_ref, gv_ref, gw_ref,
           hid, kw, maps, logs, og, gain, kbuf, vbuf, kt, qn, dn, qt, dt, stats, dqt, dq_got,
           ds_a, ds_b, w_a, own_k, own_v, term_out, term_in, dw_out, dw_in,
           ld, k_send, k_recv, v_send, v_recv, t_send, t_recv, w_send, w_recv, x_send, x_recv):
    chips = n // 2
    me = lax.axis_index("sp")
    tp = lax.axis_index("tp")
    u = me // 2
    c = me % 2
    rows = hid.shape[0]
    scale = HEAD_DIM ** (-0.5)
    partner = 2 * u + 1 - c
    width = hid.shape[1] // n

    barrier = pltpu.get_barrier_semaphore()

    def greet(i, carry):
        peer = lax.rem(me + i, n)
        pl.semaphore_signal(barrier, inc=1, device_id=(peer, tp), device_id_type=MESH_ID)
        return carry

    lax.fori_loop(1, n, greet, 0)

    my_rows = pl.ds(pl.multiple_of(c * rows, rows), rows)
    its_rows = pl.ds(pl.multiple_of((1 - c) * rows, rows), rows)
    loads = [
        pltpu.make_async_copy(kw_hbm, kw, ld.at[0]),
        pltpu.make_async_copy(hid_hbm, hid, ld.at[1]),
        pltpu.make_async_copy(val_hbm, vbuf.at[u], ld.at[2]),
        pltpu.make_async_copy(map_hbm, maps, ld.at[3]),
        pltpu.make_async_copy(og_hbm, og, ld.at[4]),
        pltpu.make_async_copy(gain_hbm, gain, ld.at[5]),
        pltpu.make_async_copy(log_hbm, logs, ld.at[6]),
        pltpu.make_async_copy(q_hbm, qn.at[my_rows, :], ld.at[7]),
    ]
    for load in (loads[2], loads[0], loads[1], loads[7], loads[3], loads[4], loads[5], loads[6]):
        load.start()

    def to(src, dst, s_sem, r_sem, device):
        return pltpu.make_async_remote_copy(
            src_ref=src, dst_ref=dst, send_sem=s_sem, recv_sem=r_sem,
            device_id=(device, tp), device_id_type=MESH_ID)

    def k_copy(slot, dest):
        return to(kbuf.at[slot], kbuf.at[slot], k_send.at[dest], k_recv.at[slot], 2 * dest + c)

    def v_copy(slot, dest):
        return to(vbuf.at[slot], vbuf.at[slot], v_send.at[dest], v_recv.at[slot], 2 * dest + c)

    def t_copy(dest, source):
        return to(term_out.at[dest], term_in.at[source], t_send.at[dest], t_recv.at[source], 2 * dest + c)

    def w_copy(dest, source):
        return to(dw_out.at[dest], dw_in.at[source], w_send.at[dest], w_recv.at[source], dest)

    loads[2].wait()
    loads[7].wait()
    pl.semaphore_wait(barrier, n - 1)

    q_swap = to(qn.at[my_rows, :], qn.at[my_rows, :], x_send.at[0], x_recv.at[0], partner)
    q_swap.start()

    def send_v(i, carry):
        v_copy(u, chips - 1 - i).start()
        return carry

    lax.fori_loop(0, chips - 1 - u, send_v, 0)

    loads[0].wait()
    loads[1].wait()
    kbuf[u] = nn(hid[...], kw[...]).astype(BF16)

    for load in loads[3:7]:
        load.wait()

    def send_k(i, carry):
        k_copy(u, chips - 1 - i).start()
        return carry

    lax.fori_loop(0, chips - 1 - u, send_k, 0)

    lane = lax.broadcasted_iota(jnp.int32, (rows, 128), 1)
    terms = jnp.zeros((rows, 128), F32)
    for h in range(heads):
        mix = mix_ref[h]
        first = maps[:, (2 * h) * V_DIM:(2 * h + 1) * V_DIM].astype(F32)
        second = maps[:, (2 * h + 1) * V_DIM:(2 * h + 2) * V_DIM].astype(F32)
        pre = first - mix * second
        inverse = lax.rsqrt(jnp.mean(pre * pre, axis=-1, keepdims=True) + NORM_EPS)
        up = og[:, h * V_DIM:(h + 1) * V_DIM].astype(F32) * gain[...] * OUT_SCALE
        d_out = inverse * (up - pre * (inverse * inverse * jnp.mean(up * pre, axis=-1, keepdims=True)))
        dn[my_rows, h * V_DIM:(h + 1) * V_DIM] = d_out.astype(BF16)
        terms = jnp.where(lane == 2 * h, jnp.sum(d_out * first, axis=-1, keepdims=True), terms)
        terms = jnp.where(lane == 2 * h + 1, jnp.sum(d_out * second, axis=-1, keepdims=True), terms)
    stats[c, 2 * heads:4 * heads] = terms.T[:2 * heads]
    mix_row = lax.broadcasted_iota(jnp.int32, (2 * heads, rows), 0)
    log_rows = logs[...] * LOG2E
    for h in range(heads):
        shift = jnp.log(jnp.full((2 * heads, rows), mix_ref[h], F32)) * LOG2E
        log_rows = jnp.where(mix_row == 2 * h + 1, log_rows - shift, log_rows)
    stats[c, :2 * heads] = log_rows

    d_swap = to(dn.at[my_rows, :], dn.at[my_rows, :], x_send.at[1], x_recv.at[1], partner)
    s_swap = to(stats.at[c], stats.at[c], x_send.at[2], x_recv.at[2], partner)
    d_swap.start()
    s_swap.start()
    dqt[...] = jnp.zeros_like(dqt)
    q_swap.wait_recv()
    for h in range(2 * heads):
        qt[h * HEAD_DIM:(h + 1) * HEAD_DIM, :] = qn[:, h * HEAD_DIM:(h + 1) * HEAD_DIM].T
    d_swap.wait_recv()
    s_swap.wait_recv()
    for h in range(heads):
        dt[h * V_DIM:(h + 1) * V_DIM, :] = dn[:, h * V_DIM:(h + 1) * V_DIM].T

    q_rows = 2 * rows

    def block(j, masked):
        kk = kbuf[j]
        kt[...] = kk.T
        vv = vbuf[j]
        both = lambda r: jnp.concatenate([stats[0, r:r + 1, :], stats[1, r:r + 1, :]], axis=1)

        def products(h):
            s_a = nn(kk[:, :HEAD_DIM], qt[(2 * h) * HEAD_DIM:(2 * h + 1) * HEAD_DIM, :])
            s_b = nn(kk[:, HEAD_DIM:], qt[(2 * h + 1) * HEAD_DIM:(2 * h + 2) * HEAD_DIM, :])
            d_p = nn(vv, dt[h * V_DIM:(h + 1) * V_DIM, :])
            return s_a, s_b, d_p

        ready = products(0)
        for h in range(heads):
            s_a, s_b, d_p = ready
            if h + 1 < heads:
                ready = products(h + 1)
            x_a = s_a * (scale * LOG2E) - both(2 * h)
            x_b = s_b * (scale * LOG2E) - both(2 * h + 1)
            if masked:
                key_at = c * rows + lax.broadcasted_iota(jnp.int32, (rows, q_rows), 0)
                query_at = lax.broadcasted_iota(jnp.int32, (rows, q_rows), 1)
                seen = key_at <= query_at
                x_a = jnp.where(seen, x_a, -1e30)
                x_b = jnp.where(seen, x_b, -1e30)
            p_a = jnp.exp2(x_a)
            p_b = jnp.exp2(x_b)
            cols = slice(h * q_rows, (h + 1) * q_rows)
            w_h = (p_a - p_b).astype(BF16)
            a_h = (p_a * (d_p - both(2 * heads + 2 * h))).astype(BF16)
            b_h = (p_b * (both(2 * heads + 2 * h + 1) - d_p)).astype(BF16)
            w_a[:, cols] = w_h
            ds_a[:, cols] = a_h
            ds_b[:, cols] = b_h
            dqt[(2 * h) * HEAD_DIM:(2 * h + 1) * HEAD_DIM, :] += nn(kt[:HEAD_DIM, :], a_h)
            dqt[(2 * h + 1) * HEAD_DIM:(2 * h + 2) * HEAD_DIM, :] += nn(kt[HEAD_DIM:, :], b_h)
        g_v = jnp.zeros((rows, V_DIM), F32)
        g_a = jnp.zeros((rows, HEAD_DIM), F32)
        g_b = jnp.zeros((rows, HEAD_DIM), F32)
        for h in range(heads):
            cols = slice(h * q_rows, (h + 1) * q_rows)
            g_a += nn(ds_a[:, cols], qn[:, (2 * h) * HEAD_DIM:(2 * h + 1) * HEAD_DIM])
            g_b += nn(ds_b[:, cols], qn[:, (2 * h + 1) * HEAD_DIM:(2 * h + 2) * HEAD_DIM])
            g_v += nn(w_a[:, cols], dn[:, h * V_DIM:(h + 1) * V_DIM])
        return g_a * scale, g_b * scale, g_v

    def step(j, carry):
        k_copy(j, u).wait_recv()
        v_copy(j, u).wait_recv()
        g_a, g_b, g_v = block(j, False)
        term_out[j, :, :HEAD_DIM] = g_a.astype(BF16)
        term_out[j, :, HEAD_DIM:2 * HEAD_DIM] = g_b.astype(BF16)
        term_out[j, :, 2 * HEAD_DIM:] = g_v.astype(BF16)
        t_copy(j, u).start()
        return carry

    lax.fori_loop(0, u, step, 0)
    g_a, g_b, g_v = block(u, True)
    own_k[:, :HEAD_DIM] = g_a
    own_k[:, HEAD_DIM:] = g_b
    own_v[...] = g_v

    dq_swap = to(dqt.at[:, its_rows], dq_got, x_send.at[3], x_recv.at[3], partner)
    dq_swap.start()

    def gather_terms(i, carry):
        t_copy(u, i).wait_recv()
        own_k[...] += term_in[i, :, :2 * HEAD_DIM].astype(F32)
        own_v[...] += term_in[i, :, 2 * HEAD_DIM:].astype(F32)
        return carry

    lax.fori_loop(u + 1, chips, gather_terms, 0)
    gk_ref[...] = own_k[...].astype(BF16)
    gv_ref[...] = own_v[...].astype(BF16)
    kt[...] = own_k[...].T.astype(BF16)

    def project(i, carry):
        chip = lax.rem(u + 1 + i, chips)
        piece = nn(kt[...], hid[:, pl.ds(pl.multiple_of(2 * width * chip, 2 * width), 2 * width)]).astype(BF16)
        dw_out[2 * chip] = piece[:, :width]
        dw_out[2 * chip + 1] = piece[:, width:]

        @pl.when(chip != u)
        def _():
            w_copy(2 * chip, me).start()
            w_copy(2 * chip + 1, me).start()

        return carry

    lax.fori_loop(0, chips, project, 0)
    w_copy(partner, me).start()

    dq_swap.wait_recv()
    for h in range(2 * heads):
        part = dqt[h * HEAD_DIM:(h + 1) * HEAD_DIM, my_rows] + dq_got[h * HEAD_DIM:(h + 1) * HEAD_DIM, :]
        gq_ref[:, h * HEAD_DIM:(h + 1) * HEAD_DIM] = (part * scale).T.astype(BF16)

    def add_piece(i, total):
        w_copy(me, i).wait_recv()
        return total + dw_in[i].astype(F32)

    total = dw_out[me].astype(F32)
    total = lax.fori_loop(0, me, add_piece, total)
    total = lax.fori_loop(me + 1, n, add_piece, total)
    gw_ref[...] = total.T

    def v_sent(i, carry):
        v_copy(u, chips - 1 - i).wait_send()
        k_copy(u, chips - 1 - i).wait_send()
        return carry

    lax.fori_loop(0, chips - 1 - u, v_sent, 0)

    def t_sent(j, carry):
        t_copy(j, u).wait_send()
        return carry

    lax.fori_loop(0, u, t_sent, 0)

    def w_sent(i, carry):
        w_copy(lax.rem(me + i, n), me).wait_send()
        return carry

    lax.fori_loop(1, n, w_sent, 0)
    for swap in (q_swap, d_swap, s_swap, dq_swap):
        swap.wait_send()


def on_device(n, hidden, key_weight, queries, values, map_out, log_sums, out_grad, mixing, out_gain):
    rows, model = hidden.shape
    heads = mixing.shape[0]
    k_cols = key_weight.shape[1]
    q_cols = queries.shape[1]
    chips = n // 2
    width = model // n
    vm = pltpu.VMEM
    dma = pltpu.SemaphoreType.DMA
    anywhere = pl.BlockSpec(memory_space=pl.ANY)
    inside = pl.BlockSpec(memory_space=pltpu.VMEM)
    return pl.pallas_call(
        functools.partial(kernel, n, heads),
        out_shape=(
            jax.ShapeDtypeStruct((rows, q_cols), BF16),
            jax.ShapeDtypeStruct((rows, k_cols), BF16),
            jax.ShapeDtypeStruct((rows, V_DIM), BF16),
            jax.ShapeDtypeStruct((width, k_cols), F32),
        ),
        in_specs=[pl.BlockSpec(memory_space=pltpu.SMEM)] + [anywhere] * 8,
        out_specs=(inside,) * 4,
        scratch_shapes=[
            vm((rows, model), BF16),
            vm((model, k_cols), BF16),
            vm((rows, 2 * heads * V_DIM), BF16),
            vm((2 * heads, rows), F32),
            vm((rows, heads * V_DIM), BF16),
            vm((1, V_DIM), F32),
            vm((chips, rows, k_cols), BF16),
            vm((chips, rows, V_DIM), BF16),
            vm((k_cols, rows), BF16),
            vm((2 * rows, q_cols), BF16),
            vm((2 * rows, heads * V_DIM), BF16),
            vm((q_cols, 2 * rows), BF16),
            vm((heads * V_DIM, 2 * rows), BF16),
            vm((2, 4 * heads, rows), F32),
            vm((q_cols, 2 * rows), F32),
            vm((q_cols, rows), F32),
            vm((rows, heads * 2 * rows), BF16),
            vm((rows, heads * 2 * rows), BF16),
            vm((rows, heads * 2 * rows), BF16),
            vm((rows, k_cols), F32),
            vm((rows, V_DIM), F32),
            vm((chips, rows, k_cols + V_DIM), BF16),
            vm((chips, rows, k_cols + V_DIM), BF16),
            vm((n, k_cols, width), BF16),
            vm((n, k_cols, width), BF16),
            dma((8,)),
            dma((chips,)),
            dma((chips,)),
            dma((chips,)),
            dma((chips,)),
            dma((chips,)),
            dma((chips,)),
            dma((n,)),
            dma((n,)),
            dma((4,)),
            dma((4,)),
        ],
        compiler_params=pltpu.CompilerParams(
            collective_id=0, has_side_effects=True, vmem_limit_bytes=62 * 1024 * 1024),
    )(mixing, hidden, key_weight, queries, values, map_out, log_sums, out_grad, out_gain.reshape(1, -1))


def solution(mesh):
    placed = (
        P("sp", None),
        P(None, "tp"),
        P("sp", "tp"),
        P("sp", "tp"),
        P("sp", "tp"),
        P("tp", "sp"),
        P("sp", "tp"),
        P("tp"),
        P(),
    )
    return jax.shard_map(
        functools.partial(on_device, mesh.shape["sp"]),
        mesh=mesh,
        in_specs=placed,
        out_specs=(P("sp", "tp"), P("sp", "tp"), P("sp", "tp"), P("sp", "tp")),
        check_vma=False,
    )
```

```python
import functools
import math

import jax
import jax.numpy as jnp
from jax import lax
from jax.experimental import pallas as pl
from jax.experimental.pallas import tpu as pltpu
from jax.sharding import PartitionSpec as P

HEAD_DIM = 128
V_DIM = 256
OUT_SCALE = 0.8
NORM_EPS = 1e-06
LOG2E = math.log2(math.e)
PLANES = 4
MESH_ID = pl.DeviceIdType.MESH
BF16 = jnp.bfloat16
F32 = jnp.float32


def nn(a, b):
    return jnp.dot(a, b, preferred_element_type=F32)


def kernel(n, heads, mix_ref, hid_hbm, kw_hbm, q_hbm, val_hbm, map_hbm, log_hbm, og_hbm, gain_hbm,
           gq_ref, gk_ref, gv_ref, gw_ref,
           hid, kw, maps, logs, og, gain, kb, vb, ktb, qn, dn, qt, dt, stats, dqt, dq_own, dq_out, dq_in,
           ds_a, ds_b, w_a, dk_sum, dv_sum, core_k, core_v, core_k_in, core_v_in, k_out, v_out, k_in, v_in,
           gkt, x_out, x_in, dw_out, dw_in,
           ld, kv_send, kv_recv, f_send, f_recv, q_send, q_recv, r_send, b_send, b_recv,
           c_send, c_recv, t_send, t_recv, y_send, y_recv, w_send, w_recv):
    chips = n // 2
    ny = chips // PLANES
    me = lax.axis_index("sp")
    tp = lax.axis_index("tp")
    u = me // 2
    c = me % 2
    z = u // ny
    y = u % ny
    rows = hid.shape[0]
    scale = HEAD_DIM ** (-0.5)
    partner = 2 * u + 1 - c
    width = hid.shape[1] // n
    passes = PLANES - 1 - z

    barrier = pltpu.get_barrier_semaphore()

    def greet(i, carry):
        peer = 2 * lax.rem(u + i, chips) + c
        pl.semaphore_signal(barrier, inc=1, device_id=(peer, tp), device_id_type=MESH_ID)
        return carry

    lax.fori_loop(1, chips, greet, 0)
    pl.semaphore_signal(barrier, inc=1, device_id=(partner, tp), device_id_type=MESH_ID)

    mine = pl.ds(pl.multiple_of(c * rows, rows), rows)
    other = pl.ds(pl.multiple_of((1 - c) * rows, rows), rows)
    loads = [
        pltpu.make_async_copy(q_hbm, qn.at[z], ld.at[0]),
        pltpu.make_async_copy(val_hbm, vb.at[y, mine, :], ld.at[1]),
        pltpu.make_async_copy(kw_hbm, kw, ld.at[2]),
        pltpu.make_async_copy(hid_hbm, hid, ld.at[3]),
        pltpu.make_async_copy(map_hbm, maps, ld.at[4]),
        pltpu.make_async_copy(og_hbm, og, ld.at[5]),
        pltpu.make_async_copy(gain_hbm, gain, ld.at[6]),
        pltpu.make_async_copy(log_hbm, logs, ld.at[7]),
    ]
    for load in loads:
        load.start()

    def to(src, dst, s_sem, r_sem, device):
        return pltpu.make_async_remote_copy(
            src_ref=src, dst_ref=dst, send_sem=s_sem, recv_sem=r_sem,
            device_id=(device, tp), device_id_type=MESH_ID)

    def at(plane, col):
        return 2 * (plane * ny + col) + c

    def kv_copy(m, buf, source, dest):
        part = buf.at[source, mine, :]
        return to(part, part, kv_send.at[m, dest], kv_recv.at[m, source], at(z, dest))

    def f_copy(m, buf, source):
        part = buf.at[source, mine, :]
        return to(part, part, f_send.at[m, source], f_recv.at[m, source], partner)

    def f_wait(m, buf, source):
        part = buf.at[source, other, :]
        to(part, part, f_send.at[m, source], f_recv.at[m, source], partner).wait_recv()

    def q_copy(m, buf, source, dest, sem):
        return to(buf.at[source], buf.at[source], sem, q_recv.at[m, source], at(dest, y))

    def b_copy(source, dest):
        return to(dq_out.at[dest], dq_in.at[source], b_send.at[dest], b_recv.at[source], at(dest, y))

    def c_copy(m, src, dst, col):
        return to(src.at[col], dst.at[col], c_send.at[m, col], c_recv.at[m, col], partner)

    def t_copy(m, src, dst, source, dest):
        return to(src.at[dest], dst.at[source], t_send.at[m, dest], t_recv.at[m, source], at(z, dest))

    def y_copy(chip):
        return to(x_out.at[chip], x_in.at[chip], y_send.at[chip], y_recv.at[chip], partner)

    def w_copy(dest, source):
        return to(dw_out.at[dest], dw_in.at[source], w_send.at[dest], w_recv.at[source], 2 * dest + c)

    def send_down(m, buf):
        @pl.when(z >= 1)
        def _():
            q_copy(m, buf, z, z - 1, q_send.at[m, 0]).start()

        @pl.when(z == PLANES - 1)
        def _():
            q_copy(m, buf, z, 0, q_send.at[m, 1]).start()

    def others(body):
        def one(i, carry):
            body(lax.rem(y + ny - i, ny))
            return carry

        lax.fori_loop(1, ny, one, 0)

    dk_sum[...] = jnp.zeros_like(dk_sum)
    dv_sum[...] = jnp.zeros_like(dv_sum)
    dqt[...] = jnp.zeros_like(dqt)
    loads[0].wait()
    loads[1].wait()
    pl.semaphore_wait(barrier, chips)
    send_down(0, qn)
    f_copy(1, vb, y).start()
    others(lambda col: kv_copy(1, vb, y, col).start())

    loads[2].wait()
    loads[3].wait()
    kb[y, mine, :] = nn(hid[...], kw[...]).astype(BF16)
    for load in loads[4:]:
        load.wait()
    f_copy(0, kb, y).start()
    others(lambda col: kv_copy(0, kb, y, col).start())

    lane = lax.broadcasted_iota(jnp.int32, (rows, 128), 1)
    terms = jnp.zeros((rows, 128), F32)
    for h in range(heads):
        mix = mix_ref[h]
        first = maps[:, (2 * h) * V_DIM:(2 * h + 1) * V_DIM].astype(F32)
        second = maps[:, (2 * h + 1) * V_DIM:(2 * h + 2) * V_DIM].astype(F32)
        pre = first - mix * second
        inverse = lax.rsqrt(jnp.mean(pre * pre, axis=-1, keepdims=True) + NORM_EPS)
        up = og[:, h * V_DIM:(h + 1) * V_DIM].astype(F32) * gain[...] * OUT_SCALE
        d_out = inverse * (up - pre * (inverse * inverse * jnp.mean(up * pre, axis=-1, keepdims=True)))
        dn[z, :, h * V_DIM:(h + 1) * V_DIM] = d_out.astype(BF16)
        terms = jnp.where(lane == 2 * h, jnp.sum(d_out * first, axis=-1, keepdims=True), terms)
        terms = jnp.where(lane == 2 * h + 1, jnp.sum(d_out * second, axis=-1, keepdims=True), terms)
    stats[z, 2 * heads:4 * heads] = terms.T[:2 * heads]
    mix_row = lax.broadcasted_iota(jnp.int32, (2 * heads, rows), 0)
    log_rows = logs[...] * LOG2E
    for h in range(heads):
        shift = jnp.log(jnp.full((2 * heads, rows), mix_ref[h], F32)) * LOG2E
        log_rows = jnp.where(mix_row == 2 * h + 1, log_rows - shift, log_rows)
    stats[z, :2 * heads] = log_rows

    send_down(1, dn)

    @pl.when(z == PLANES - 1)
    def _():
        q_copy(1, dn, z, 1, q_send.at[1, 2]).start()

    def s_copy(source, dest):
        return q_copy(2, stats, source, dest, q_send.at[2, dest])

    def send_stats(dest, carry):
        s_copy(z, dest).start()
        return carry

    lax.fori_loop(0, z, send_stats, 0)

    def turn(plane):
        for h in range(2 * heads):
            qt[h * HEAD_DIM:(h + 1) * HEAD_DIM, :] = qn[plane, :, h * HEAD_DIM:(h + 1) * HEAD_DIM].T
        for h in range(heads):
            dt[h * V_DIM:(h + 1) * V_DIM, :] = dn[plane, :, h * V_DIM:(h + 1) * V_DIM].T

    k_rows = 2 * rows

    def block(col, plane, masked):
        def products(h):
            kk = kb.at[col]
            s_a = nn(kk[:, :HEAD_DIM], qt[(2 * h) * HEAD_DIM:(2 * h + 1) * HEAD_DIM, :])
            s_b = nn(kk[:, HEAD_DIM:], qt[(2 * h + 1) * HEAD_DIM:(2 * h + 2) * HEAD_DIM, :])
            d_p = nn(vb[col], dt[h * V_DIM:(h + 1) * V_DIM, :])
            return s_a, s_b, d_p

        ready = products(0)
        for h in range(heads):
            s_a, s_b, d_p = ready
            if h + 1 < heads:
                ready = products(h + 1)
            x_a = s_a * (scale * LOG2E) - stats[plane, 2 * h:2 * h + 1, :]
            x_b = s_b * (scale * LOG2E) - stats[plane, 2 * h + 1:2 * h + 2, :]
            if masked:
                key_at = lax.broadcasted_iota(jnp.int32, (k_rows, rows), 0)
                query_at = c * rows + lax.broadcasted_iota(jnp.int32, (k_rows, rows), 1)
                seen = key_at <= query_at
                x_a = jnp.where(seen, x_a, -1e30)
                x_b = jnp.where(seen, x_b, -1e30)
            p_a = jnp.exp2(x_a)
            p_b = jnp.exp2(x_b)
            cols = slice(h * rows, (h + 1) * rows)
            a_h = (p_a * (d_p - stats[plane, 2 * heads + 2 * h:2 * heads + 2 * h + 1, :])).astype(BF16)
            b_h = (p_b * (stats[plane, 2 * heads + 2 * h + 1:2 * heads + 2 * h + 2, :] - d_p)).astype(BF16)
            w_a[:, cols] = (p_a - p_b).astype(BF16)
            ds_a[:, cols] = a_h
            ds_b[:, cols] = b_h
            dqt[(2 * h) * HEAD_DIM:(2 * h + 1) * HEAD_DIM, :] += nn(ktb[col, :HEAD_DIM, :], a_h)
            dqt[(2 * h + 1) * HEAD_DIM:(2 * h + 2) * HEAD_DIM, :] += nn(ktb[col, HEAD_DIM:, :], b_h)
        g_v = jnp.zeros((k_rows, V_DIM), F32)
        g_a = jnp.zeros((k_rows, HEAD_DIM), F32)
        g_b = jnp.zeros((k_rows, HEAD_DIM), F32)
        for h in range(heads):
            cols = slice(h * rows, (h + 1) * rows)
            g_a += nn(ds_a[:, cols], qn[plane, :, (2 * h) * HEAD_DIM:(2 * h + 1) * HEAD_DIM])
            g_b += nn(ds_b[:, cols], qn[plane, :, (2 * h + 1) * HEAD_DIM:(2 * h + 2) * HEAD_DIM])
            g_v += nn(w_a[:, cols], dn[plane, :, h * V_DIM:(h + 1) * V_DIM])
        dk_sum[col, :, :HEAD_DIM] += g_a
        dk_sum[col, :, HEAD_DIM:] += g_b
        dv_sum[col] += g_v

    turn(z)
    f_wait(0, kb, y)
    f_wait(1, vb, y)
    ktb[y] = kb[y].T
    block(y, z, True)

    def take(i, carry):
        col = lax.rem(y + ny - i, ny)
        for m, buf in ((0, kb), (1, vb)):
            kv_copy(m, buf, col, y).wait_recv()
            f_copy(m, buf, col).start()
        for m, buf in ((0, kb), (1, vb)):
            f_wait(m, buf, col)
        ktb[col] = kb[col].T

        @pl.when(col < y)
        def _():
            block(col, z, False)

        return carry

    lax.fori_loop(1, ny, take, 0)
    dq_own[...] = dqt[...]

    def to_partner(col):
        core_k[col] = dk_sum[col, other, :].astype(BF16)
        c_copy(0, core_k, core_k_in, col).start()
        core_v[col] = dv_sum[col, other, :].astype(BF16)
        c_copy(1, core_v, core_v_in, col).start()

    def to_owner(col):
        c_copy(0, core_k, core_k_in, col).wait_recv()
        k_out[col] = (dk_sum[col, mine, :] + core_k_in[col].astype(F32)).astype(BF16)
        t_copy(0, k_out, k_in, y, col).start()
        c_copy(1, core_v, core_v_in, col).wait_recv()
        v_out[col] = (dv_sum[col, mine, :] + core_v_in[col].astype(F32)).astype(BF16)
        t_copy(1, v_out, v_in, y, col).start()

    def one_pass(p, carry):
        plane = jnp.where((z == 0) & (p >= 2), PLANES + 1 - p, z + p)
        q_copy(0, qn, plane, z, q_send.at[0, 0]).wait_recv()

        @pl.when((z >= 1) & (p == 1) & (z <= PLANES - 2))
        def _():
            q_copy(0, qn, plane, z - 1, r_send.at[0]).start()

        q_copy(1, dn, plane, z, q_send.at[1, 0]).wait_recv()

        @pl.when((z == 1) & (p == 1))
        def _():
            q_copy(1, dn, plane, z - 1, r_send.at[1]).start()

        q_copy(2, stats, plane, z, q_send.at[2, 0]).wait_recv()
        turn(plane)
        dqt[...] = jnp.zeros_like(dqt)

        def one(i, inner):
            col = lax.rem(y + i, ny)
            block(col, plane, False)

            @pl.when(p == passes)
            def _():
                @pl.when(i > 1)
                def _():
                    to_owner(lax.rem(y + i - 1, ny))

                to_partner(col)

            return inner

        lax.fori_loop(1, ny + 1, one, 0)
        dq_out[plane] = dqt[...].astype(BF16)
        b_copy(z, plane).start()
        return carry

    lax.fori_loop(1, passes + 1, one_pass, 0)

    @pl.when(passes == 0)
    def _():
        def give(col, carry):
            to_partner(col)
            return carry

        lax.fori_loop(0, y + 1, give, 0)

        def pass_on(col, carry):
            to_owner(col)
            return carry

        lax.fori_loop(0, y, pass_on, 0)

    c_copy(0, core_k, core_k_in, y).wait_recv()
    gk = dk_sum[y, mine, :] + core_k_in[y].astype(F32)
    first_in = jnp.where(passes == 0, y + 1, 0)

    def add_k(col, total):
        t_copy(0, k_out, k_in, col, y).wait_recv()
        return total + k_in[col].astype(F32)

    gk = lax.fori_loop(first_in, y, add_k, gk)
    gk = lax.fori_loop(y + 1, ny, add_k, gk) * scale
    gk_ref[...] = gk.astype(BF16)
    gkt[...] = gk.T.astype(BF16)

    def project(i, carry):
        chip = lax.rem(u + 1 + i, chips)
        piece = nn(gkt[...], hid[:, pl.ds(pl.multiple_of(2 * width * chip, 2 * width), 2 * width)])
        low, high = piece[:, :width], piece[:, width:]
        dw_out[chip] = jnp.where(c == 0, low, high).astype(BF16)
        x_out[chip] = jnp.where(c == 0, high, low).astype(BF16)
        y_copy(chip).start()
        return carry

    lax.fori_loop(0, chips, project, 0)

    def spread(i, carry):
        chip = lax.rem(u + 1 + i, chips)
        y_copy(chip).wait_recv()
        dw_out[chip] = (dw_out[chip].astype(F32) + x_in[chip].astype(F32)).astype(BF16)

        @pl.when(chip != u)
        def _():
            w_copy(chip, u).start()

        return carry

    lax.fori_loop(0, chips, spread, 0)

    c_copy(1, core_v, core_v_in, y).wait_recv()
    gv = dv_sum[y, mine, :] + core_v_in[y].astype(F32)

    def add_v(col, total):
        t_copy(1, v_out, v_in, col, y).wait_recv()
        return total + v_in[col].astype(F32)

    gv = lax.fori_loop(first_in, y, add_v, gv)
    gv = lax.fori_loop(y + 1, ny, add_v, gv)
    gv_ref[...] = gv.astype(BF16)

    def add_q(plane, carry):
        b_copy(plane, z).wait_recv()
        dq_own[...] += dq_in[plane].astype(F32)
        return carry

    lax.fori_loop(0, z, add_q, 0)
    for h in range(2 * heads):
        part = dq_own[h * HEAD_DIM:(h + 1) * HEAD_DIM, :]
        gq_ref[:, h * HEAD_DIM:(h + 1) * HEAD_DIM] = (part * scale).T.astype(BF16)

    def add_w(i, total):
        chip = chips - 1 - i
        w_copy(u, chip).wait_recv()
        return total + dw_in[chip].astype(F32)

    total = dw_out[u].astype(F32)
    total = lax.fori_loop(0, chips - 1 - u, add_w, total)
    total = lax.fori_loop(chips - u, chips, add_w, total)
    gw_ref[...] = total.T

    for m, buf in ((0, kb), (1, vb)):
        f_copy(m, buf, y).wait_send()

    def sent(col):
        for m, buf in ((0, kb), (1, vb)):
            kv_copy(m, buf, y, col).wait_send()
            f_copy(m, buf, col).wait_send()

    others(sent)

    @pl.when(z >= 1)
    def _():
        q_copy(0, qn, z, 0, q_send.at[0, 0]).wait_send()
        q_copy(1, dn, z, 0, q_send.at[1, 0]).wait_send()

    @pl.when(z == PLANES - 1)
    def _():
        q_copy(0, qn, z, 0, q_send.at[0, 1]).wait_send()
        q_copy(1, dn, z, 0, q_send.at[1, 1]).wait_send()
        q_copy(1, dn, z, 0, q_send.at[1, 2]).wait_send()

    @pl.when((z >= 1) & (z <= PLANES - 2))
    def _():
        q_copy(0, qn, z + 1, z - 1, r_send.at[0]).wait_send()

    @pl.when(z == 1)
    def _():
        q_copy(1, dn, z + 1, z - 1, r_send.at[1]).wait_send()

    def stats_sent(dest, carry):
        s_copy(z, dest).wait_send()
        return carry

    lax.fori_loop(0, z, stats_sent, 0)

    def back_sent(plane, carry):
        b_copy(z, plane).wait_send()
        return carry

    lax.fori_loop(z + 1, PLANES, back_sent, 0)
    last_in = jnp.where(passes == 0, y + 1, ny)

    def terms_sent(col, carry):
        for m, src, dst in ((0, core_k, core_k_in), (1, core_v, core_v_in)):
            c_copy(m, src, dst, col).wait_send()

        @pl.when(col != y)
        def _():
            t_copy(0, k_out, k_in, y, col).wait_send()
            t_copy(1, v_out, v_in, y, col).wait_send()

        return carry

    lax.fori_loop(0, last_in, terms_sent, 0)

    def dw_sent(chip, carry):
        y_copy(chip).wait_send()

        @pl.when(chip != u)
        def _():
            w_copy(chip, u).wait_send()

        return carry

    lax.fori_loop(0, chips, dw_sent, 0)


def on_device(n, hidden, key_weight, queries, values, map_out, log_sums, out_grad, mixing, out_gain):
    rows, model = hidden.shape
    heads = mixing.shape[0]
    k_cols = key_weight.shape[1]
    q_cols = queries.shape[1]
    chips = n // 2
    ny = chips // PLANES
    width = model // n
    vm = pltpu.VMEM
    dma = pltpu.SemaphoreType.DMA
    anywhere = pl.BlockSpec(memory_space=pl.ANY)
    inside = pl.BlockSpec(memory_space=pltpu.VMEM)
    tall = vm((2 * rows, heads * rows), BF16)
    slots = vm((ny, rows, k_cols), BF16)
    return pl.pallas_call(
        functools.partial(kernel, n, heads),
        out_shape=(
            jax.ShapeDtypeStruct((rows, q_cols), BF16),
            jax.ShapeDtypeStruct((rows, k_cols), BF16),
            jax.ShapeDtypeStruct((rows, V_DIM), BF16),
            jax.ShapeDtypeStruct((width, k_cols), F32),
        ),
        in_specs=[pl.BlockSpec(memory_space=pltpu.SMEM)] + [anywhere] * 8,
        out_specs=(inside,) * 4,
        scratch_shapes=[
            vm((rows, model), BF16),
            vm((model, k_cols), BF16),
            vm((rows, 2 * heads * V_DIM), BF16),
            vm((2 * heads, rows), F32),
            vm((rows, heads * V_DIM), BF16),
            vm((1, V_DIM), F32),
            vm((ny, 2 * rows, k_cols), BF16),
            vm((ny, 2 * rows, V_DIM), BF16),
            vm((ny, k_cols, 2 * rows), BF16),
            vm((PLANES, rows, q_cols), BF16),
            vm((PLANES, rows, heads * V_DIM), BF16),
            vm((q_cols, rows), BF16),
            vm((heads * V_DIM, rows), BF16),
            vm((PLANES, 4 * heads, rows), F32),
            vm((q_cols, rows), F32),
            vm((q_cols, rows), F32),
            vm((PLANES, q_cols, rows), BF16),
            vm((PLANES, q_cols, rows), BF16),
            tall, tall, tall,
            vm((ny, 2 * rows, k_cols), F32),
            vm((ny, 2 * rows, V_DIM), F32),
            slots, slots, slots, slots, slots, slots, slots, slots,
            vm((k_cols, rows), BF16),
            vm((chips, k_cols, width), BF16),
            vm((chips, k_cols, width), BF16),
            vm((chips, k_cols, width), BF16),
            vm((chips, k_cols, width), BF16),
            dma((8,)),
            dma((2, ny)), dma((2, ny)),
            dma((2, ny)), dma((2, ny)),
            dma((3, PLANES)), dma((3, PLANES)), dma((2,)),
            dma((PLANES,)), dma((PLANES,)),
            dma((2, ny)), dma((2, ny)),
            dma((2, ny)), dma((2, ny)),
            dma((chips,)), dma((chips,)),
            dma((chips,)), dma((chips,)),
        ],
        compiler_params=pltpu.CompilerParams(
            collective_id=0, has_side_effects=True, vmem_limit_bytes=63 * 1024 * 1024),
    )(mixing, hidden, key_weight, queries, values, map_out, log_sums, out_grad, out_gain.reshape(1, -1))


def solution(mesh):
    placed = (
        P("sp", None),
        P(None, "tp"),
        P("sp", "tp"),
        P("sp", "tp"),
        P("sp", "tp"),
        P("tp", "sp"),
        P("sp", "tp"),
        P("tp"),
        P(),
    )
    return jax.shard_map(
        functools.partial(on_device, mesh.shape["sp"]),
        mesh=mesh,
        in_specs=placed,
        out_specs=(P("sp", "tp"), P("sp", "tp"), P("sp", "tp"), P("sp", "tp")),
        check_vma=False,
    )
```

```python
import functools
import math

import jax
import jax.numpy as jnp
from jax import lax
from jax.experimental import pallas as pl
from jax.experimental.pallas import tpu as pltpu
from jax.sharding import PartitionSpec as P

HEAD_DIM = 128
V_DIM = 256
OUT_SCALE = 0.8
NORM_EPS = 1e-06
LOG2E = math.log2(math.e)
PLANES = 4
LAG = 3
MESH_ID = pl.DeviceIdType.MESH
BF16 = jnp.bfloat16
F32 = jnp.float32


def nn(a, b):
    return jnp.dot(a, b, preferred_element_type=F32)


def write_out(a, b, c, d, a_out, b_out, c_out, d_out, sem):
    copies = [pltpu.make_async_copy(src, dst, sem.at[i])
              for i, (src, dst) in enumerate(((a, a_out), (b, b_out), (c, c_out), (d, d_out)))]
    for copy in copies:
        copy.start()
    for copy in copies:
        copy.wait()


def kernel(n, heads, mix_ref, hid_hbm, kw_hbm, q_hbm, val_hbm, map_hbm, log_hbm, og_hbm, gain_hbm,
           gq_ref, gk_ref, gv_ref, gw_ref,
           hid, kw, maps, logs, og, gain, kb, vb, ktb, qn, dn, qt, dt, stats, dqt, dq_own, dq_out, dq_in,
           ds_a, ds_b, w_a, dk_sum, dv_sum, core_k, core_v, core_k_in, core_v_in, k_out, v_out, k_in, v_in,
           gkt, x_out, x_in, dw_out, dw_in, e_out, e_in, own_k, own_v, ring_in,
           ld, kv_send, kv_recv, f_send, f_recv, q_send, q_recv, r_send, b_send, b_recv,
           c_send, c_recv, t_send, t_recv, y_send, y_recv, w_send, w_recv,
           h_send, h_recv, e_send, e_recv, g_send, g_recv, p_send, p_recv):
    chips = n // 2
    ny = chips // PLANES
    ring = ny == 4
    me = lax.axis_index("sp")
    tp = lax.axis_index("tp")
    u = me // 2
    c = me % 2
    z = u // ny
    y = u % ny
    rows = hid.shape[0]
    scale = HEAD_DIM ** (-0.5)
    partner = 2 * u + 1 - c
    width = hid.shape[1] // n
    odd = lax.rem(z, 2) == 1
    top = z == PLANES - 1
    low = z < PLANES // 2
    n_q = jnp.where(z == 0, 2, jnp.where(z == PLANES - 1, 0, 1))
    above = jnp.where(low, 2 * z + 1, z)
    below = lax.div(z, 2)

    barrier = pltpu.get_barrier_semaphore()

    def greet(i, carry):
        peer = 2 * lax.rem(u + i, chips) + c
        pl.semaphore_signal(barrier, inc=1, device_id=(peer, tp), device_id_type=MESH_ID)
        return carry

    lax.fori_loop(1, chips, greet, 0)
    pl.semaphore_signal(barrier, inc=1, device_id=(partner, tp), device_id_type=MESH_ID)

    mine = pl.ds(pl.multiple_of(c * rows, rows), rows)
    other = pl.ds(pl.multiple_of((1 - c) * rows, rows), rows)
    loads = [
        pltpu.make_async_copy(q_hbm, qn.at[z], ld.at[0]),
        pltpu.make_async_copy(map_hbm, maps, ld.at[1]),
        pltpu.make_async_copy(og_hbm, og, ld.at[2]),
        pltpu.make_async_copy(gain_hbm, gain, ld.at[3]),
        pltpu.make_async_copy(log_hbm, logs, ld.at[4]),
        pltpu.make_async_copy(val_hbm, vb.at[y, mine, :], ld.at[5]),
        pltpu.make_async_copy(kw_hbm, kw, ld.at[6]),
        pltpu.make_async_copy(hid_hbm, hid, ld.at[7]),
    ]
    for load in loads:
        load.start()

    def to(src, dst, s_sem, r_sem, device):
        return pltpu.make_async_remote_copy(
            src_ref=src, dst_ref=dst, send_sem=s_sem, recv_sem=r_sem,
            device_id=(device, tp), device_id_type=MESH_ID)

    def at(plane, col):
        return 2 * (plane * ny + col) + c

    def kv_copy(m, buf, source, dest):
        part = buf.at[source, mine, :]
        return to(part, part, kv_send.at[m, source - y + dest], kv_recv.at[m, source], at(z, dest))

    def kv_wait(m, buf, slot):
        part = buf.at[slot, mine, :]
        to(part, part, kv_send.at[m, 0], kv_recv.at[m, slot], me).wait_recv()

    def turned(step):
        return lax.rem(y + step, ny)

    def g_copy(m, buf, s, step):
        part = buf.at[s * ny + turned(4 - step), mine, :]
        return to(part, part, g_send.at[m, s], kv_recv.at[m, s * ny + turned(4 - step)], at(z, turned(step)))

    def p_copy(m, src, s, step):
        return to(src.at[s * ny + turned(2)], ring_in.at[m, s], p_send.at[m, s], p_recv.at[m, s],
                  at(z, turned(step)))

    def near(body):
        if ring:
            body(turned(1))
            body(turned(3))
        else:
            others(body)

    def h_copy(m, buf):
        return to(buf.at[y, mine, :], buf.at[ny + y, mine, :], h_send.at[m], h_recv.at[m], at(above, y))

    def e_copy(m):
        return to(e_out.at[m], e_in.at[m], e_send.at[m], e_recv.at[m], at(below, y))

    def f_copy(m, buf, source):
        part = buf.at[source, mine, :]
        return to(part, part, f_send.at[m, source], f_recv.at[m, source], partner)

    def f_wait(m, buf, source):
        part = buf.at[source, other, :]
        to(part, part, f_send.at[m, source], f_recv.at[m, source], partner).wait_recv()

    def q_copy(m, buf, source, dest, sem):
        return to(buf.at[source], buf.at[source], sem, q_recv.at[m, source], at(dest, y))

    def b_copy(source, dest):
        return to(dq_out.at[dest], dq_in.at[source], b_send.at[dest], b_recv.at[source], at(dest, y))

    def c_copy(m, src, dst, col):
        return to(src.at[col], dst.at[col], c_send.at[m, col], c_recv.at[m, col], partner)

    def t_copy(m, src, dst, base, source, dest):
        return to(src.at[base + dest], dst.at[base + source], t_send.at[m, base + dest],
                  t_recv.at[m, base + source], at(z, dest))

    def y_copy(chip):
        return to(x_out.at[chip], x_in.at[chip], y_send.at[chip], y_recv.at[chip], partner)

    def w_copy(dest, source):
        return to(dw_out.at[dest], dw_in.at[source], w_send.at[dest], w_recv.at[source], 2 * dest + c)

    def send_down(m, buf):
        @pl.when(z >= 2)
        def _():
            q_copy(m, buf, z, z - 1, q_send.at[m, 0]).start()

        @pl.when(z == PLANES - 1)
        def _():
            q_copy(m, buf, z, 0, q_send.at[m, 1]).start()

    def others(body):
        def one(i, carry):
            body(lax.rem(y + ny - i, ny))
            return carry

        lax.fori_loop(1, ny, one, 0)

    dk_sum[...] = jnp.zeros_like(dk_sum)
    dv_sum[...] = jnp.zeros_like(dv_sum)
    dqt[...] = jnp.zeros_like(dqt)
    loads[0].wait()
    pl.semaphore_wait(barrier, chips)
    send_down(0, qn)
    for load in loads[1:5]:
        load.wait()

    lane = lax.broadcasted_iota(jnp.int32, (rows, 128), 1)
    terms = jnp.zeros((rows, 128), F32)
    for h in range(heads):
        mix = mix_ref[h]
        first = maps[:, (2 * h) * V_DIM:(2 * h + 1) * V_DIM].astype(F32)
        second = maps[:, (2 * h + 1) * V_DIM:(2 * h + 2) * V_DIM].astype(F32)
        pre = first - mix * second
        inverse = lax.rsqrt(jnp.mean(pre * pre, axis=-1, keepdims=True) + NORM_EPS)
        up = og[:, h * V_DIM:(h + 1) * V_DIM].astype(F32) * gain[...] * OUT_SCALE
        d_out = inverse * (up - pre * (inverse * inverse * jnp.mean(up * pre, axis=-1, keepdims=True)))
        dn[z, :, h * V_DIM:(h + 1) * V_DIM] = d_out.astype(BF16)
        terms = jnp.where(lane == 2 * h, jnp.sum(d_out * first, axis=-1, keepdims=True), terms)
        terms = jnp.where(lane == 2 * h + 1, jnp.sum(d_out * second, axis=-1, keepdims=True), terms)
    stats[z, 2 * heads:4 * heads] = terms.T[:2 * heads]
    mix_row = lax.broadcasted_iota(jnp.int32, (2 * heads, rows), 0)
    log_rows = logs[...] * LOG2E
    for h in range(heads):
        shift = jnp.log(jnp.full((2 * heads, rows), mix_ref[h], F32)) * LOG2E
        log_rows = jnp.where(mix_row == 2 * h + 1, log_rows - shift, log_rows)
    stats[z, :2 * heads] = log_rows

    send_down(1, dn)

    @pl.when(z >= 2)
    def _():
        q_copy(2, stats, z, z - 1, q_send.at[2, 1]).start()
        q_copy(2, stats, z, 0, q_send.at[2, 0]).start()

    def share(m, buf):
        f_copy(m, buf, y).start()

        @pl.when(low)
        def _():
            h_copy(m, buf).start()

        near(lambda col: kv_copy(m, buf, y, col).start())

    loads[5].wait()
    share(1, vb)
    loads[6].wait()
    loads[7].wait()
    kb[y, mine, :] = nn(hid[...], kw[...]).astype(BF16)
    share(0, kb)

    def turn(plane):
        for h in range(2 * heads):
            qt[h * HEAD_DIM:(h + 1) * HEAD_DIM, :] = qn[plane, :, h * HEAD_DIM:(h + 1) * HEAD_DIM].T
        for h in range(heads):
            dt[h * V_DIM:(h + 1) * V_DIM, :] = dn[plane, :, h * V_DIM:(h + 1) * V_DIM].T

    k_rows = 2 * rows

    def block(col, plane, masked):
        def products(h):
            kk = kb.at[col]
            s_a = nn(kk[:, :HEAD_DIM], qt[(2 * h) * HEAD_DIM:(2 * h + 1) * HEAD_DIM, :])
            s_b = nn(kk[:, HEAD_DIM:], qt[(2 * h + 1) * HEAD_DIM:(2 * h + 2) * HEAD_DIM, :])
            d_p = nn(vb[col], dt[h * V_DIM:(h + 1) * V_DIM, :])
            return s_a, s_b, d_p

        ready = products(0)
        for h in range(heads):
            s_a, s_b, d_p = ready
            if h + 1 < heads:
                ready = products(h + 1)
            x_a = s_a * (scale * LOG2E) - stats[plane, 2 * h:2 * h + 1, :]
            x_b = s_b * (scale * LOG2E) - stats[plane, 2 * h + 1:2 * h + 2, :]
            if masked:
                key_at = lax.broadcasted_iota(jnp.int32, (k_rows, rows), 0)
                query_at = c * rows + lax.broadcasted_iota(jnp.int32, (k_rows, rows), 1)
                seen = key_at <= query_at
                x_a = jnp.where(seen, x_a, -1e30)
                x_b = jnp.where(seen, x_b, -1e30)
            p_a = jnp.exp2(x_a)
            p_b = jnp.exp2(x_b)
            cols = slice(h * rows, (h + 1) * rows)
            a_h = (p_a * (d_p - stats[plane, 2 * heads + 2 * h:2 * heads + 2 * h + 1, :])).astype(BF16)
            b_h = (p_b * (stats[plane, 2 * heads + 2 * h + 1:2 * heads + 2 * h + 2, :] - d_p)).astype(BF16)
            w_a[:, cols] = (p_a - p_b).astype(BF16)
            ds_a[:, cols] = a_h
            ds_b[:, cols] = b_h
            dqt[(2 * h) * HEAD_DIM:(2 * h + 1) * HEAD_DIM, :] += nn(ktb[col, :HEAD_DIM, :], a_h)
            dqt[(2 * h + 1) * HEAD_DIM:(2 * h + 2) * HEAD_DIM, :] += nn(ktb[col, HEAD_DIM:, :], b_h)
        g_v = jnp.zeros((k_rows, V_DIM), F32)
        g_a = jnp.zeros((k_rows, HEAD_DIM), F32)
        g_b = jnp.zeros((k_rows, HEAD_DIM), F32)
        for h in range(heads):
            cols = slice(h * rows, (h + 1) * rows)
            g_a += nn(ds_a[:, cols], qn[plane, :, (2 * h) * HEAD_DIM:(2 * h + 1) * HEAD_DIM])
            g_b += nn(ds_b[:, cols], qn[plane, :, (2 * h + 1) * HEAD_DIM:(2 * h + 2) * HEAD_DIM])
            g_v += nn(w_a[:, cols], dn[plane, :, h * V_DIM:(h + 1) * V_DIM])
        dk_sum[col, :, :HEAD_DIM] += g_a
        dk_sum[col, :, HEAD_DIM:] += g_b
        dv_sum[col] += g_v

    turn(z)
    f_wait(0, kb, y)
    f_wait(1, vb, y)
    ktb[y] = kb[y].T
    block(y, z, True)

    def pass_down(m, buf):
        q_copy(m, buf, z + 1, z, q_send.at[m, 0]).wait_recv()
        q_copy(m, buf, z + 1, z - 1, r_send.at[m]).start()

    def receive(slot):
        for m, buf in ((0, kb), (1, vb)):
            kv_wait(m, buf, slot)
            f_copy(m, buf, slot).start()

    def ready_slot(slot):
        for m, buf in ((0, kb), (1, vb)):
            f_wait(m, buf, slot)
        ktb[slot] = kb[slot].T

    def pass_round(s):
        if ring:
            for m, buf, step in ((0, kb, 3), (1, vb, 1)):
                kv_wait(m, buf, s * ny + turned(4 - step))
                g_copy(m, buf, s, step).start()
                f_copy(m, buf, s * ny + turned(4 - step)).start()
            for m, buf, step in ((0, kb, 3), (1, vb, 1)):
                kv_wait(m, buf, s * ny + turned(step))
                f_copy(m, buf, s * ny + turned(step)).start()

    def far(i):
        if ring:
            return turned(jnp.where(i == 1, 3, jnp.where(i == 2, 1, 2)))
        return turned(ny - i)

    def got(i, slot):
        if ring:
            @pl.when(i == 3)
            def _():
                receive(slot)
        else:
            receive(slot)

    def last_order(i):
        if ring:
            return turned(jnp.where(i == 1, 2, jnp.where(i == 2, 1, jnp.where(i == 3, 3, 0))))
        return turned(i)

    @pl.when(z == 1)
    def _():
        pass_down(0, qn)

    pass_round(0)

    @pl.when(odd)
    def _():
        for m, buf in ((0, kb), (1, vb)):
            to(buf.at[y, mine, :], buf.at[ny + y, mine, :], h_send.at[m], h_recv.at[m], partner).wait_recv()
            f_copy(m, buf, ny + y).start()
            near(lambda col: kv_copy(m, buf, ny + y, col).start())

    def take(i, carry):
        col = far(i)
        got(i, col)
        ready_slot(col)

        @pl.when(col < y)
        def _():
            block(col, z, False)

        return carry

    lax.fori_loop(1, ny, take, 0)
    dq_own[...] = dqt[...]

    @pl.when(odd)
    def _():
        pass_round(1)

    def to_partner(slot):
        core_k[slot] = dk_sum[slot, other, :].astype(BF16)
        c_copy(0, core_k, core_k_in, slot).start()
        core_v[slot] = dv_sum[slot, other, :].astype(BF16)
        c_copy(1, core_v, core_v_in, slot).start()

    def to_owner(base, col):
        slot = base + col
        c_copy(0, core_k, core_k_in, slot).wait_recv()
        k_out[slot] = (dk_sum[slot, mine, :] + core_k_in[slot].astype(F32)).astype(BF16)
        t_copy(0, k_out, k_in, base, y, col).start()
        c_copy(1, core_v, core_v_in, slot).wait_recv()
        v_out[slot] = (dv_sum[slot, mine, :] + core_v_in[slot].astype(F32)).astype(BF16)
        t_copy(1, v_out, v_in, base, y, col).start()

    def to_ring(s, col):
        slot = s * ny + col
        back = lax.rem(col - y + ny, ny)
        for m, sums, core, core_in, out, arrived, step in (
                (0, dk_sum, core_k, core_k_in, k_out, k_in, 3), (1, dv_sum, core_v, core_v_in, v_out, v_in, 1)):
            c_copy(m, core, core_in, slot).wait_recv()
            term = sums[slot, mine, :] + core_in[slot].astype(F32)

            @pl.when(back == step)
            def _():
                p_copy(m, out, s, 4 - step).wait_recv()
                out[slot] = (term + ring_in[m, s].astype(F32)).astype(BF16)

            @pl.when(back != step)
            def _():
                out[slot] = term.astype(BF16)

            @pl.when(back == 2)
            def _():
                p_copy(m, out, s, step).start()

            @pl.when(back != 2)
            def _():
                t_copy(m, out, arrived, s * ny, y, col).start()

    def hand_over(s, col):
        if ring:
            to_ring(s, col)
        else:
            to_owner(s * ny, col)

    @pl.when(top)
    def _():
        def give(col, carry):
            to_partner(col)
            return carry

        lax.fori_loop(0, y + 1, give, 0)

        def pass_on(col, carry):
            to_owner(0, col)
            return carry

        lax.fori_loop(0, y, pass_on, 0)

    first_in = jnp.where(top, y + 1, 0)

    def collect(m, sums, core_in, arrived, src, base, first, whole):
        slot = base + y
        c_copy(m, src, core_in, slot).wait_recv()
        total = sums[slot, mine, :] + core_in[slot].astype(F32)

        def add(col, total):
            t_copy(m, src, arrived, base, col, y).wait_recv()
            return total + arrived[base + col].astype(F32)

        if ring and whole:
            return add(turned(3), add(turned(1), total))
        total = lax.fori_loop(first, y, add, total)
        return lax.fori_loop(y + 1, ny, add, total)

    def extra():
        turn(z)
        dqt[...] = jnp.zeros_like(dqt)

        def one(i, carry):
            col = turned(jnp.where(i == 0, 0, jnp.where(i == 1, 2, jnp.where(i == 2, 1, 3)))) if ring else turned(i)
            prev = turned(jnp.where(i == 2, 2, 1)) if ring else turned(i - 1)
            slot = ny + col

            if ring:
                @pl.when(i == 1)
                def _():
                    receive(slot)
            else:
                @pl.when(i > 0)
                def _():
                    receive(slot)

            @pl.when((z == 1) & (i == 1 % ny))
            def _():
                pass_down(1, dn)

            ready_slot(slot)
            block(slot, z, False)

            @pl.when(i > 1)
            def _():
                hand_over(1, prev)

            to_partner(slot)
            return carry

        lax.fori_loop(0, ny, one, 0)
        if ny > 1:
            hand_over(1, turned(ny - 1))
        dq_own[...] += dqt[...]
        e_out[0] = collect(0, dk_sum, core_k_in, k_in, core_k, ny, 0, True).astype(BF16)
        e_copy(0).start()
        e_out[1] = collect(1, dv_sum, core_v_in, v_in, core_v, ny, 0, True).astype(BF16)
        e_copy(1).start()

    @pl.when(odd)
    def _():
        extra()

    def one_pass(p, carry):
        plane = jnp.where(z == 0, PLANES - p, z + 1)

        @pl.when(z != 1)
        def _():
            q_copy(0, qn, plane, z, q_send.at[0, 0]).wait_recv()
            q_copy(1, dn, plane, z, q_send.at[1, 0]).wait_recv()

        q_copy(2, stats, plane, z, q_send.at[2, 0]).wait_recv()
        turn(plane)
        dqt[...] = jnp.zeros_like(dqt)

        def one(i, inner):
            col = last_order(i)
            block(col, plane, False)

            @pl.when(p == n_q)
            def _():
                @pl.when(i > 1)
                def _():
                    hand_over(0, last_order(i - 1))

                to_partner(col)

            return inner

        lax.fori_loop(1, ny + 1, one, 0)
        dq_out[plane] = dqt[...].astype(BF16)
        b_copy(z, plane).start()
        return carry

    lax.fori_loop(1, n_q + 1, one_pass, 0)
    def finish_keys(whole):
        gk = collect(0, dk_sum, core_k_in, k_in, core_k, 0, first_in, whole)
        own_k[...] = gk

        @pl.when(low)
        def _():
            to(e_out.at[0], e_in.at[0], e_send.at[0], e_recv.at[0], partner).wait_recv()
            own_k[...] += e_in[0].astype(F32)

        gk = own_k[...] * scale
        gk_ref[...] = gk.astype(BF16)
        gkt[...] = gk.T.astype(BF16)

        def spread(chip):
            y_copy(chip).wait_recv()
            dw_out[chip] = (dw_out[chip].astype(F32) + x_in[chip].astype(F32)).astype(BF16)

            @pl.when(chip != u)
            def _():
                w_copy(chip, u).start()

        def project(i, carry):
            @pl.when(i < chips)
            def _():
                chip = lax.rem(u + 1 + i, chips)
                piece = nn(gkt[...], hid[:, pl.ds(pl.multiple_of(2 * width * chip, 2 * width), 2 * width)])
                left, right = piece[:, :width], piece[:, width:]
                dw_out[chip] = jnp.where(c == 0, left, right).astype(BF16)
                x_out[chip] = jnp.where(c == 0, right, left).astype(BF16)
                y_copy(chip).start()

            @pl.when(i >= LAG)
            def _():
                spread(lax.rem(u + 1 + i - LAG, chips))

            return carry

        lax.fori_loop(0, chips + LAG, project, 0)
        own_v[...] = collect(1, dv_sum, core_v_in, v_in, core_v, 0, first_in, whole)

        @pl.when(low)
        def _():
            to(e_out.at[1], e_in.at[1], e_send.at[1], e_recv.at[1], partner).wait_recv()
            own_v[...] += e_in[1].astype(F32)

        gv_ref[...] = own_v[...].astype(BF16)

    @pl.when(top)
    def _():
        finish_keys(False)

    @pl.when(jnp.logical_not(top))
    def _():
        finish_keys(True)

    def add_q(plane, carry):
        b_copy(plane, z).wait_recv()
        dq_own[...] += dq_in[plane].astype(F32)
        return carry

    @pl.when(z >= 2)
    def _():
        add_q(z - 1, 0)
        add_q(0, 0)

    for h in range(2 * heads):
        part = dq_own[h * HEAD_DIM:(h + 1) * HEAD_DIM, :]
        gq_ref[:, h * HEAD_DIM:(h + 1) * HEAD_DIM] = (part * scale).T.astype(BF16)

    def add_w(i, total):
        chip = chips - 1 - i
        w_copy(u, chip).wait_recv()
        return total + dw_in[chip].astype(F32)

    total = dw_out[u].astype(F32)
    total = lax.fori_loop(0, chips - 1 - u, add_w, total)
    total = lax.fori_loop(chips - u, chips, add_w, total)
    gw_ref[...] = total.T

    def kv_sent(base):
        for m, buf in ((0, kb), (1, vb)):
            f_copy(m, buf, base + y).wait_send()

        def sent(col):
            for m, buf in ((0, kb), (1, vb)):
                kv_copy(m, buf, base + y, col).wait_send()

        near(sent)

        def forwarded(col):
            for m, buf in ((0, kb), (1, vb)):
                f_copy(m, buf, base + col).wait_send()

        others(forwarded)
        if ring:
            for m, buf, step in ((0, kb, 3), (1, vb, 1)):
                g_copy(m, buf, 1 if base else 0, step).wait_send()

    kv_sent(0)

    @pl.when(odd)
    def _():
        kv_sent(ny)
        e_copy(0).wait_send()
        e_copy(1).wait_send()

    @pl.when(low)
    def _():
        h_copy(0, kb).wait_send()
        h_copy(1, vb).wait_send()

    @pl.when(z >= 2)
    def _():
        for m, buf in ((0, qn), (1, dn), (2, stats)):
            q_copy(m, buf, z, 0, q_send.at[m, 0]).wait_send()
        q_copy(2, stats, z, 0, q_send.at[2, 1]).wait_send()

    @pl.when(top)
    def _():
        q_copy(0, qn, z, 0, q_send.at[0, 1]).wait_send()
        q_copy(1, dn, z, 0, q_send.at[1, 1]).wait_send()

    @pl.when(z == 1)
    def _():
        q_copy(0, qn, z + 1, 0, r_send.at[0]).wait_send()
        q_copy(1, dn, z + 1, 0, r_send.at[1]).wait_send()

    def back_sent(p, carry):
        b_copy(z, jnp.where(z == 0, PLANES - p, z + 1)).wait_send()
        return carry

    lax.fori_loop(1, n_q + 1, back_sent, 0)

    def all_terms_sent(base, count, skipped):
        def terms_sent(col, carry):
            for m, src, dst in ((0, core_k, core_k_in), (1, core_v, core_v_in)):
                c_copy(m, src, dst, base + col).wait_send()

            @pl.when((col != y) & (col != skipped))
            def _():
                t_copy(0, k_out, k_in, base, y, col).wait_send()
                t_copy(1, v_out, v_in, base, y, col).wait_send()

            return carry

        lax.fori_loop(0, count, terms_sent, 0)

    def ring_sent(s):
        if ring:
            p_copy(0, k_out, s, 3).wait_send()
            p_copy(1, v_out, s, 1).wait_send()

    all_terms_sent(0, jnp.where(top, y + 1, ny), jnp.where(top, ny, turned(2)) if ring else ny)

    @pl.when(jnp.logical_not(top))
    def _():
        ring_sent(0)

    @pl.when(odd)
    def _():
        all_terms_sent(ny, ny, turned(2) if ring else ny)
        ring_sent(1)

    def dw_sent(chip, carry):
        y_copy(chip).wait_send()

        @pl.when(chip != u)
        def _():
            w_copy(chip, u).wait_send()

        return carry

    lax.fori_loop(0, chips, dw_sent, 0)


def on_device(n, hidden, key_weight, queries, values, map_out, log_sums, out_grad, mixing, out_gain):
    rows, model = hidden.shape
    heads = mixing.shape[0]
    k_cols = key_weight.shape[1]
    q_cols = queries.shape[1]
    chips = n // 2
    ny = chips // PLANES
    width = model // n
    vm = pltpu.VMEM
    dma = pltpu.SemaphoreType.DMA
    anywhere = pl.BlockSpec(memory_space=pl.ANY)
    inside = pl.BlockSpec(memory_space=pltpu.VMEM)
    tall = vm((2 * rows, heads * rows), BF16)
    slots = vm((2 * ny, rows, k_cols), BF16)
    results = pl.pallas_call(
        functools.partial(kernel, n, heads),
        out_shape=(
            jax.ShapeDtypeStruct((rows, q_cols), BF16),
            jax.ShapeDtypeStruct((rows, k_cols), BF16),
            jax.ShapeDtypeStruct((rows, V_DIM), BF16),
            jax.ShapeDtypeStruct((width, k_cols), F32),
        ),
        in_specs=[pl.BlockSpec(memory_space=pltpu.SMEM)] + [anywhere] * 8,
        out_specs=(inside,) * 4,
        scratch_shapes=[
            vm((rows, model), BF16),
            vm((model, k_cols), BF16),
            vm((rows, 2 * heads * V_DIM), BF16),
            vm((2 * heads, rows), F32),
            vm((rows, heads * V_DIM), BF16),
            vm((1, V_DIM), F32),
            vm((2 * ny, 2 * rows, k_cols), BF16),
            vm((2 * ny, 2 * rows, V_DIM), BF16),
            vm((2 * ny, k_cols, 2 * rows), BF16),
            vm((PLANES, rows, q_cols), BF16),
            vm((PLANES, rows, heads * V_DIM), BF16),
            vm((q_cols, rows), BF16),
            vm((heads * V_DIM, rows), BF16),
            vm((PLANES, 4 * heads, rows), F32),
            vm((q_cols, rows), F32),
            vm((q_cols, rows), F32),
            vm((PLANES, q_cols, rows), BF16),
            vm((PLANES, q_cols, rows), BF16),
            tall, tall, tall,
            vm((2 * ny, 2 * rows, k_cols), F32),
            vm((2 * ny, 2 * rows, V_DIM), F32),
            slots, slots, slots, slots, slots, slots, slots, slots,
            vm((k_cols, rows), BF16),
            vm((chips, k_cols, width), BF16),
            vm((chips, k_cols, width), BF16),
            vm((chips, k_cols, width), BF16),
            vm((chips, k_cols, width), BF16),
            vm((2, rows, k_cols), BF16),
            vm((2, rows, k_cols), BF16),
            vm((rows, k_cols), F32),
            vm((rows, V_DIM), F32),
            vm((2, 2, rows, k_cols), BF16),
            dma((8,)),
            dma((2, 2 * ny)), dma((2, 2 * ny)),
            dma((2, 2 * ny)), dma((2, 2 * ny)),
            dma((3, PLANES)), dma((3, PLANES)), dma((2,)),
            dma((PLANES,)), dma((PLANES,)),
            dma((2, 2 * ny)), dma((2, 2 * ny)),
            dma((2, 2 * ny)), dma((2, 2 * ny)),
            dma((chips,)), dma((chips,)),
            dma((chips,)), dma((chips,)),
            dma((2,)), dma((2,)),
            dma((2,)), dma((2,)),
            dma((2, 2)), dma((2, 2)),
            dma((2, 2)), dma((2, 2)),
        ],
        compiler_params=pltpu.CompilerParams(
            collective_id=0, has_side_effects=True, vmem_limit_bytes=63 * 1024 * 1024),
    )(mixing, hidden, key_weight, queries, values, map_out, log_sums, out_grad, out_gain.reshape(1, -1))
    return pl.pallas_call(
        write_out,
        out_shape=tuple(jax.ShapeDtypeStruct(r.shape, r.dtype) for r in results),
        in_specs=[inside] * 4,
        out_specs=(anywhere,) * 4,
        scratch_shapes=[dma((4,))],
    )(*results)


def solution(mesh):
    placed = (
        P("sp", None),
        P(None, "tp"),
        P("sp", "tp"),
        P("sp", "tp"),
        P("sp", "tp"),
        P("tp", "sp"),
        P("sp", "tp"),
        P("tp"),
        P(),
    )
    return jax.shard_map(
        functools.partial(on_device, mesh.shape["sp"]),
        mesh=mesh,
        in_specs=placed,
        out_specs=(P("sp", "tp"), P("sp", "tp"), P("sp", "tp"), P("sp", "tp")),
        check_vma=False,
    )
```

```python
import functools
import math

import jax
import jax.numpy as jnp
from jax import lax
from jax.experimental import pallas as pl
from jax.experimental.pallas import tpu as pltpu
from jax.sharding import PartitionSpec as P

HEAD_DIM = 128
V_DIM = 256
OUT_SCALE = 0.8
NORM_EPS = 1e-06
LOG2E = math.log2(math.e)
PLANES = 4
LAG = 3
MESH_ID = pl.DeviceIdType.MESH
BF16 = jnp.bfloat16
F32 = jnp.float32


def nn(a, b):
    return jnp.dot(a, b, preferred_element_type=F32)


def write_out(a, b, c, d, a_out, b_out, c_out, d_out, sem):
    copies = [pltpu.make_async_copy(src, dst, sem.at[i])
              for i, (src, dst) in enumerate(((a, a_out), (b, b_out), (c, c_out), (d, d_out)))]
    for copy in copies:
        copy.start()
    for copy in copies:
        copy.wait()


def kernel(n, heads, mix_ref, hid_hbm, kw_hbm, q_hbm, val_hbm, map_hbm, log_hbm, og_hbm, gain_hbm,
           gq_ref, gk_ref, gv_ref, gw_ref,
           hid, kw, maps, logs, og, gain, kb, vb, ktb, qn, dn, qt, dt, stats, dqt, dq_own, dq_out, dq_in,
           ds_a, ds_b, w_a, dk_sum, dv_sum, core_k, core_v, core_k_in, core_v_in, k_out, v_out, k_in, v_in,
           gkt, x_out, x_in, dw_out, dw_in, e_out, e_in, own_k, own_v, ring_in,
           ld, kv_send, kv_recv, f_send, f_recv, q_send, q_recv, r_send, b_send, b_recv,
           c_send, c_recv, t_send, t_recv, y_send, y_recv, w_send, w_recv,
           h_send, h_recv, e_send, e_recv, g_send, g_recv, p_send, p_recv):
    chips = n // 2
    ny = chips // PLANES
    ring = ny == 4
    me = lax.axis_index("sp")
    tp = lax.axis_index("tp")
    u = me // 2
    c = me % 2
    z = u // ny
    y = u % ny
    rows = hid.shape[0]
    scale = HEAD_DIM ** (-0.5)
    partner = 2 * u + 1 - c
    width = hid.shape[1] // n
    odd = lax.rem(z, 2) == 1
    top = z == PLANES - 1
    low = z < PLANES // 2
    n_q = jnp.where(z == 0, 2, jnp.where(z == PLANES - 1, 0, 1))
    above = jnp.where(low, 2 * z + 1, z)
    below = lax.div(z, 2)

    barrier = pltpu.get_barrier_semaphore()

    def greet(i, carry):
        peer = 2 * lax.rem(u + i, chips) + c
        pl.semaphore_signal(barrier, inc=1, device_id=(peer, tp), device_id_type=MESH_ID)
        return carry

    lax.fori_loop(1, chips, greet, 0)
    pl.semaphore_signal(barrier, inc=1, device_id=(partner, tp), device_id_type=MESH_ID)

    mine = pl.ds(pl.multiple_of(c * rows, rows), rows)
    other = pl.ds(pl.multiple_of((1 - c) * rows, rows), rows)
    loads = [
        pltpu.make_async_copy(q_hbm, qn.at[z], ld.at[0]),
        pltpu.make_async_copy(map_hbm, maps, ld.at[1]),
        pltpu.make_async_copy(og_hbm, og, ld.at[2]),
        pltpu.make_async_copy(gain_hbm, gain, ld.at[3]),
        pltpu.make_async_copy(log_hbm, logs, ld.at[4]),
        pltpu.make_async_copy(val_hbm, vb.at[y, mine, :], ld.at[5]),
        pltpu.make_async_copy(kw_hbm, kw, ld.at[6]),
        pltpu.make_async_copy(hid_hbm, hid, ld.at[7]),
    ]
    for load in loads:
        load.start()

    def to(src, dst, s_sem, r_sem, device):
        return pltpu.make_async_remote_copy(
            src_ref=src, dst_ref=dst, send_sem=s_sem, recv_sem=r_sem,
            device_id=(device, tp), device_id_type=MESH_ID)

    def at(plane, col):
        return 2 * (plane * ny + col) + c

    def kv_copy(m, buf, source, dest):
        part = buf.at[source, mine, :]
        return to(part, part, kv_send.at[m, source - y + dest], kv_recv.at[m, source], at(z, dest))

    def kv_wait(m, buf, slot):
        part = buf.at[slot, mine, :]
        to(part, part, kv_send.at[m, 0], kv_recv.at[m, slot], me).wait_recv()

    def turned(step):
        return lax.rem(y + step, ny)

    def g_copy(m, buf, s, step):
        part = buf.at[s * ny + turned(4 - step), mine, :]
        return to(part, part, g_send.at[m, s], kv_recv.at[m, s * ny + turned(4 - step)], at(z, turned(step)))

    def p_copy(m, src, s, step):
        return to(src.at[s * ny + turned(2)], ring_in.at[m, s], p_send.at[m, s], p_recv.at[m, s],
                  at(z, turned(step)))

    def near(body):
        if ring:
            body(turned(1))
            body(turned(3))
        else:
            others(body)

    def h_copy(m, buf):
        return to(buf.at[y, mine, :], buf.at[ny + y, mine, :], h_send.at[m], h_recv.at[m], at(above, y))

    def e_copy(m):
        return to(e_out.at[m], e_in.at[m], e_send.at[m], e_recv.at[m], at(below, y))

    def f_copy(m, buf, source):
        part = buf.at[source, mine, :]
        return to(part, part, f_send.at[m, source], f_recv.at[m, source], partner)

    def f_wait(m, buf, source):
        part = buf.at[source, other, :]
        to(part, part, f_send.at[m, source], f_recv.at[m, source], partner).wait_recv()

    def q_copy(m, buf, source, dest, sem):
        return to(buf.at[source], buf.at[source], sem, q_recv.at[m, source], at(dest, y))

    def b_copy(source, dest):
        return to(dq_out.at[dest], dq_in.at[source], b_send.at[dest], b_recv.at[source], at(dest, y))

    def back_copy(plane):
        via = (z == 0) & (plane == PLANES - 2)
        slot = jnp.where(via, 1, z)
        return to(dq_out.at[plane], dq_in.at[slot], b_send.at[plane], b_recv.at[slot],
                  at(jnp.where(via, PLANES - 1, plane), y))

    def relay_copy():
        return to(dq_in.at[1], dq_in.at[0], b_send.at[0], b_recv.at[0], at(PLANES - 2, y))

    def c_copy(m, src, dst, col):
        return to(src.at[col], dst.at[col], c_send.at[m, col], c_recv.at[m, col], partner)

    def t_copy(m, src, dst, base, source, dest):
        return to(src.at[base + dest], dst.at[base + source], t_send.at[m, base + dest],
                  t_recv.at[m, base + source], at(z, dest))

    def y_copy(chip):
        return to(x_out.at[chip], x_in.at[chip], y_send.at[chip], y_recv.at[chip], partner)

    def w_copy(dest, source):
        return to(dw_out.at[dest], dw_in.at[source], w_send.at[dest], w_recv.at[source], 2 * dest + c)

    def send_down(m, buf):
        @pl.when(z >= 2)
        def _():
            q_copy(m, buf, z, z - 1, q_send.at[m, 0]).start()

        @pl.when(z == PLANES - 1)
        def _():
            q_copy(m, buf, z, 0, q_send.at[m, 1]).start()

    def others(body):
        def one(i, carry):
            body(lax.rem(y + ny - i, ny))
            return carry

        lax.fori_loop(1, ny, one, 0)

    dk_sum[...] = jnp.zeros_like(dk_sum)
    dv_sum[...] = jnp.zeros_like(dv_sum)
    dqt[...] = jnp.zeros_like(dqt)
    loads[0].wait()
    pl.semaphore_wait(barrier, chips)
    send_down(0, qn)
    for load in loads[1:5]:
        load.wait()

    lane = lax.broadcasted_iota(jnp.int32, (rows, 128), 1)
    terms = jnp.zeros((rows, 128), F32)
    for h in range(heads):
        mix = mix_ref[h]
        first = maps[:, (2 * h) * V_DIM:(2 * h + 1) * V_DIM].astype(F32)
        second = maps[:, (2 * h + 1) * V_DIM:(2 * h + 2) * V_DIM].astype(F32)
        pre = first - mix * second
        inverse = lax.rsqrt(jnp.mean(pre * pre, axis=-1, keepdims=True) + NORM_EPS)
        up = og[:, h * V_DIM:(h + 1) * V_DIM].astype(F32) * gain[...] * OUT_SCALE
        d_out = inverse * (up - pre * (inverse * inverse * jnp.mean(up * pre, axis=-1, keepdims=True)))
        dn[z, :, h * V_DIM:(h + 1) * V_DIM] = d_out.astype(BF16)
        terms = jnp.where(lane == 2 * h, jnp.sum(d_out * first, axis=-1, keepdims=True), terms)
        terms = jnp.where(lane == 2 * h + 1, jnp.sum(d_out * second, axis=-1, keepdims=True), terms)
    stats[z, 2 * heads:4 * heads] = terms.T[:2 * heads]
    mix_row = lax.broadcasted_iota(jnp.int32, (2 * heads, rows), 0)
    log_rows = logs[...] * LOG2E
    for h in range(heads):
        shift = jnp.log(jnp.full((2 * heads, rows), mix_ref[h], F32)) * LOG2E
        log_rows = jnp.where(mix_row == 2 * h + 1, log_rows - shift, log_rows)
    stats[z, :2 * heads] = log_rows

    send_down(1, dn)

    @pl.when(z >= 2)
    def _():
        q_copy(2, stats, z, z - 1, q_send.at[2, 1]).start()
        q_copy(2, stats, z, 0, q_send.at[2, 0]).start()

    def share(m, buf):
        f_copy(m, buf, y).start()

        @pl.when(low)
        def _():
            h_copy(m, buf).start()

        near(lambda col: kv_copy(m, buf, y, col).start())

    loads[5].wait()
    share(1, vb)
    loads[6].wait()
    loads[7].wait()
    kb[y, mine, :] = nn(hid[...], kw[...]).astype(BF16)
    share(0, kb)

    def turn(plane):
        for h in range(2 * heads):
            qt[h * HEAD_DIM:(h + 1) * HEAD_DIM, :] = qn[plane, :, h * HEAD_DIM:(h + 1) * HEAD_DIM].T
        for h in range(heads):
            dt[h * V_DIM:(h + 1) * V_DIM, :] = dn[plane, :, h * V_DIM:(h + 1) * V_DIM].T

    k_rows = 2 * rows

    def block(col, plane, masked):
        def products(h):
            kk = kb.at[col]
            s_a = nn(kk[:, :HEAD_DIM], qt[(2 * h) * HEAD_DIM:(2 * h + 1) * HEAD_DIM, :])
            s_b = nn(kk[:, HEAD_DIM:], qt[(2 * h + 1) * HEAD_DIM:(2 * h + 2) * HEAD_DIM, :])
            d_p = nn(vb[col], dt[h * V_DIM:(h + 1) * V_DIM, :])
            return s_a, s_b, d_p

        ready = products(0)
        for h in range(heads):
            s_a, s_b, d_p = ready
            if h + 1 < heads:
                ready = products(h + 1)
            x_a = s_a * (scale * LOG2E) - stats[plane, 2 * h:2 * h + 1, :]
            x_b = s_b * (scale * LOG2E) - stats[plane, 2 * h + 1:2 * h + 2, :]
            if masked:
                key_at = lax.broadcasted_iota(jnp.int32, (k_rows, rows), 0)
                query_at = c * rows + lax.broadcasted_iota(jnp.int32, (k_rows, rows), 1)
                seen = key_at <= query_at
                x_a = jnp.where(seen, x_a, -1e30)
                x_b = jnp.where(seen, x_b, -1e30)
            p_a = jnp.exp2(x_a)
            p_b = jnp.exp2(x_b)
            cols = slice(h * rows, (h + 1) * rows)
            a_h = (p_a * (d_p - stats[plane, 2 * heads + 2 * h:2 * heads + 2 * h + 1, :])).astype(BF16)
            b_h = (p_b * (stats[plane, 2 * heads + 2 * h + 1:2 * heads + 2 * h + 2, :] - d_p)).astype(BF16)
            w_a[:, cols] = (p_a - p_b).astype(BF16)
            ds_a[:, cols] = a_h
            ds_b[:, cols] = b_h
            dqt[(2 * h) * HEAD_DIM:(2 * h + 1) * HEAD_DIM, :] += nn(ktb[col, :HEAD_DIM, :], a_h)
            dqt[(2 * h + 1) * HEAD_DIM:(2 * h + 2) * HEAD_DIM, :] += nn(ktb[col, HEAD_DIM:, :], b_h)
        g_v = jnp.zeros((k_rows, V_DIM), F32)
        g_a = jnp.zeros((k_rows, HEAD_DIM), F32)
        g_b = jnp.zeros((k_rows, HEAD_DIM), F32)
        for h in range(heads):
            cols = slice(h * rows, (h + 1) * rows)
            g_a += nn(ds_a[:, cols], qn[plane, :, (2 * h) * HEAD_DIM:(2 * h + 1) * HEAD_DIM])
            g_b += nn(ds_b[:, cols], qn[plane, :, (2 * h + 1) * HEAD_DIM:(2 * h + 2) * HEAD_DIM])
            g_v += nn(w_a[:, cols], dn[plane, :, h * V_DIM:(h + 1) * V_DIM])
        dk_sum[col, :, :HEAD_DIM] += g_a
        dk_sum[col, :, HEAD_DIM:] += g_b
        dv_sum[col] += g_v

    turn(z)
    f_wait(0, kb, y)
    f_wait(1, vb, y)
    ktb[y] = kb[y].T
    block(y, z, True)

    def pass_down(m, buf):
        q_copy(m, buf, z + 1, z, q_send.at[m, 0]).wait_recv()
        q_copy(m, buf, z + 1, z - 1, r_send.at[m]).start()

    def receive(slot):
        for m, buf in ((0, kb), (1, vb)):
            kv_wait(m, buf, slot)
            f_copy(m, buf, slot).start()

    def ready_slot(slot):
        for m, buf in ((0, kb), (1, vb)):
            f_wait(m, buf, slot)
        ktb[slot] = kb[slot].T

    def pass_round(s):
        if ring:
            for m, buf, step in ((0, kb, 3), (1, vb, 1)):
                kv_wait(m, buf, s * ny + turned(4 - step))
                g_copy(m, buf, s, step).start()
                f_copy(m, buf, s * ny + turned(4 - step)).start()
            for m, buf, step in ((0, kb, 3), (1, vb, 1)):
                kv_wait(m, buf, s * ny + turned(step))
                f_copy(m, buf, s * ny + turned(step)).start()

    def far(i):
        if ring:
            return turned(jnp.where(i == 1, 3, jnp.where(i == 2, 1, 2)))
        return turned(ny - i)

    def got(i, slot):
        if ring:
            @pl.when(i == 3)
            def _():
                receive(slot)
        else:
            receive(slot)

    def last_order(i):
        if ring:
            return turned(jnp.where(i == 1, 2, jnp.where(i == 2, 1, jnp.where(i == 3, 3, 0))))
        return turned(i)

    @pl.when(z == 1)
    def _():
        pass_down(0, qn)

    pass_round(0)

    @pl.when(odd)
    def _():
        for m, buf in ((0, kb), (1, vb)):
            to(buf.at[y, mine, :], buf.at[ny + y, mine, :], h_send.at[m], h_recv.at[m], partner).wait_recv()
            f_copy(m, buf, ny + y).start()
            near(lambda col: kv_copy(m, buf, ny + y, col).start())

    def take(i, carry):
        col = far(i)
        got(i, col)
        ready_slot(col)

        @pl.when(col < y)
        def _():
            block(col, z, False)

        return carry

    lax.fori_loop(1, ny, take, 0)
    dq_own[...] = dqt[...]

    @pl.when(odd)
    def _():
        pass_round(1)

    def to_partner(slot):
        core_k[slot] = dk_sum[slot, other, :].astype(BF16)
        c_copy(0, core_k, core_k_in, slot).start()
        core_v[slot] = dv_sum[slot, other, :].astype(BF16)
        c_copy(1, core_v, core_v_in, slot).start()

    def to_owner(base, col):
        slot = base + col
        c_copy(0, core_k, core_k_in, slot).wait_recv()
        k_out[slot] = (dk_sum[slot, mine, :] + core_k_in[slot].astype(F32)).astype(BF16)
        t_copy(0, k_out, k_in, base, y, col).start()
        c_copy(1, core_v, core_v_in, slot).wait_recv()
        v_out[slot] = (dv_sum[slot, mine, :] + core_v_in[slot].astype(F32)).astype(BF16)
        t_copy(1, v_out, v_in, base, y, col).start()

    def to_ring(s, col):
        slot = s * ny + col
        back = lax.rem(col - y + ny, ny)
        for m, sums, core, core_in, out, arrived, step in (
                (0, dk_sum, core_k, core_k_in, k_out, k_in, 3), (1, dv_sum, core_v, core_v_in, v_out, v_in, 1)):
            c_copy(m, core, core_in, slot).wait_recv()
            term = sums[slot, mine, :] + core_in[slot].astype(F32)

            @pl.when(back == step)
            def _():
                p_copy(m, out, s, 4 - step).wait_recv()
                out[slot] = (term + ring_in[m, s].astype(F32)).astype(BF16)

            @pl.when(back != step)
            def _():
                out[slot] = term.astype(BF16)

            @pl.when(back == 2)
            def _():
                p_copy(m, out, s, step).start()

            @pl.when(back != 2)
            def _():
                t_copy(m, out, arrived, s * ny, y, col).start()

    def hand_over(s, col):
        if ring:
            to_ring(s, col)
        else:
            to_owner(s * ny, col)

    @pl.when(top)
    def _():
        def give(col, carry):
            to_partner(col)
            return carry

        lax.fori_loop(0, y + 1, give, 0)

        def pass_on(col, carry):
            to_owner(0, col)
            return carry

        lax.fori_loop(0, y, pass_on, 0)

    first_in = jnp.where(top, y + 1, 0)

    def collect(m, sums, core_in, arrived, src, base, first, whole):
        slot = base + y
        c_copy(m, src, core_in, slot).wait_recv()
        total = sums[slot, mine, :] + core_in[slot].astype(F32)

        def add(col, total):
            t_copy(m, src, arrived, base, col, y).wait_recv()
            return total + arrived[base + col].astype(F32)

        if ring and whole:
            return add(turned(3), add(turned(1), total))
        total = lax.fori_loop(first, y, add, total)
        return lax.fori_loop(y + 1, ny, add, total)

    def extra():
        turn(z)
        dqt[...] = jnp.zeros_like(dqt)

        def one(i, carry):
            col = turned(jnp.where(i == 0, 0, jnp.where(i == 1, 2, jnp.where(i == 2, 1, 3)))) if ring else turned(i)
            prev = turned(jnp.where(i == 2, 2, 1)) if ring else turned(i - 1)
            slot = ny + col

            if ring:
                @pl.when(i == 1)
                def _():
                    receive(slot)
            else:
                @pl.when(i > 0)
                def _():
                    receive(slot)

            @pl.when((z == 1) & (i == 1 % ny))
            def _():
                pass_down(1, dn)

            ready_slot(slot)
            block(slot, z, False)

            @pl.when(i > 1)
            def _():
                hand_over(1, prev)

            to_partner(slot)
            return carry

        lax.fori_loop(0, ny, one, 0)
        if ny > 1:
            hand_over(1, turned(ny - 1))
        dq_own[...] += dqt[...]
        e_out[0] = collect(0, dk_sum, core_k_in, k_in, core_k, ny, 0, True).astype(BF16)
        e_copy(0).start()
        e_out[1] = collect(1, dv_sum, core_v_in, v_in, core_v, ny, 0, True).astype(BF16)
        e_copy(1).start()

    @pl.when(odd)
    def _():
        extra()

    def one_pass(p, carry):
        plane = jnp.where(z == 0, PLANES - p, z + 1)

        @pl.when(z != 1)
        def _():
            q_copy(0, qn, plane, z, q_send.at[0, 0]).wait_recv()
            q_copy(1, dn, plane, z, q_send.at[1, 0]).wait_recv()

        q_copy(2, stats, plane, z, q_send.at[2, 0]).wait_recv()
        turn(plane)
        dqt[...] = jnp.zeros_like(dqt)

        def one(i, inner):
            col = last_order(i)
            block(col, plane, False)

            @pl.when(p == n_q)
            def _():
                @pl.when(i > 1)
                def _():
                    hand_over(0, last_order(i - 1))

                to_partner(col)

            return inner

        lax.fori_loop(1, ny + 1, one, 0)
        dq_out[plane] = dqt[...].astype(BF16)
        back_copy(plane).start()
        return carry

    lax.fori_loop(1, n_q + 1, one_pass, 0)
    def finish_keys(whole):
        gk = collect(0, dk_sum, core_k_in, k_in, core_k, 0, first_in, whole)
        own_k[...] = gk

        @pl.when(low)
        def _():
            to(e_out.at[0], e_in.at[0], e_send.at[0], e_recv.at[0], partner).wait_recv()
            own_k[...] += e_in[0].astype(F32)

        gk = own_k[...] * scale
        gk_ref[...] = gk.astype(BF16)
        gkt[...] = gk.T.astype(BF16)

        def spread(chip):
            y_copy(chip).wait_recv()
            dw_out[chip] = (dw_out[chip].astype(F32) + x_in[chip].astype(F32)).astype(BF16)

            @pl.when(chip != u)
            def _():
                w_copy(chip, u).start()

        def project(i, carry):
            @pl.when(i < chips)
            def _():
                chip = lax.rem(u + 1 + i, chips)
                piece = nn(gkt[...], hid[:, pl.ds(pl.multiple_of(2 * width * chip, 2 * width), 2 * width)])
                left, right = piece[:, :width], piece[:, width:]
                dw_out[chip] = jnp.where(c == 0, left, right).astype(BF16)
                x_out[chip] = jnp.where(c == 0, right, left).astype(BF16)
                y_copy(chip).start()

            @pl.when(i >= LAG)
            def _():
                spread(lax.rem(u + 1 + i - LAG, chips))

            return carry

        lax.fori_loop(0, chips + LAG, project, 0)
        own_v[...] = collect(1, dv_sum, core_v_in, v_in, core_v, 0, first_in, whole)

        @pl.when(low)
        def _():
            to(e_out.at[1], e_in.at[1], e_send.at[1], e_recv.at[1], partner).wait_recv()
            own_v[...] += e_in[1].astype(F32)

        gv_ref[...] = own_v[...].astype(BF16)

    @pl.when(top)
    def _():
        finish_keys(False)
        b_copy(1, z).wait_recv()
        relay_copy().start()

    @pl.when(jnp.logical_not(top))
    def _():
        finish_keys(True)

    def add_q(plane, carry):
        b_copy(plane, z).wait_recv()
        dq_own[...] += dq_in[plane].astype(F32)
        return carry

    @pl.when(z >= 2)
    def _():
        add_q(z - 1, 0)
        add_q(0, 0)

    for h in range(2 * heads):
        part = dq_own[h * HEAD_DIM:(h + 1) * HEAD_DIM, :]
        gq_ref[:, h * HEAD_DIM:(h + 1) * HEAD_DIM] = (part * scale).T.astype(BF16)

    def add_w(i, total):
        chip = chips - 1 - i
        w_copy(u, chip).wait_recv()
        return total + dw_in[chip].astype(F32)

    total = dw_out[u].astype(F32)
    total = lax.fori_loop(0, chips - 1 - u, add_w, total)
    total = lax.fori_loop(chips - u, chips, add_w, total)
    gw_ref[...] = total.T

    def kv_sent(base):
        for m, buf in ((0, kb), (1, vb)):
            f_copy(m, buf, base + y).wait_send()

        def sent(col):
            for m, buf in ((0, kb), (1, vb)):
                kv_copy(m, buf, base + y, col).wait_send()

        near(sent)

        def forwarded(col):
            for m, buf in ((0, kb), (1, vb)):
                f_copy(m, buf, base + col).wait_send()

        others(forwarded)
        if ring:
            for m, buf, step in ((0, kb, 3), (1, vb, 1)):
                g_copy(m, buf, 1 if base else 0, step).wait_send()

    kv_sent(0)

    @pl.when(odd)
    def _():
        kv_sent(ny)
        e_copy(0).wait_send()
        e_copy(1).wait_send()

    @pl.when(low)
    def _():
        h_copy(0, kb).wait_send()
        h_copy(1, vb).wait_send()

    @pl.when(z >= 2)
    def _():
        for m, buf in ((0, qn), (1, dn), (2, stats)):
            q_copy(m, buf, z, 0, q_send.at[m, 0]).wait_send()
        q_copy(2, stats, z, 0, q_send.at[2, 1]).wait_send()

    @pl.when(top)
    def _():
        q_copy(0, qn, z, 0, q_send.at[0, 1]).wait_send()
        q_copy(1, dn, z, 0, q_send.at[1, 1]).wait_send()
        relay_copy().wait_send()

    @pl.when(z == 1)
    def _():
        q_copy(0, qn, z + 1, 0, r_send.at[0]).wait_send()
        q_copy(1, dn, z + 1, 0, r_send.at[1]).wait_send()

    def back_sent(p, carry):
        back_copy(jnp.where(z == 0, PLANES - p, z + 1)).wait_send()
        return carry

    lax.fori_loop(1, n_q + 1, back_sent, 0)

    def all_terms_sent(base, count, skipped):
        def terms_sent(col, carry):
            for m, src, dst in ((0, core_k, core_k_in), (1, core_v, core_v_in)):
                c_copy(m, src, dst, base + col).wait_send()

            @pl.when((col != y) & (col != skipped))
            def _():
                t_copy(0, k_out, k_in, base, y, col).wait_send()
                t_copy(1, v_out, v_in, base, y, col).wait_send()

            return carry

        lax.fori_loop(0, count, terms_sent, 0)

    def ring_sent(s):
        if ring:
            p_copy(0, k_out, s, 3).wait_send()
            p_copy(1, v_out, s, 1).wait_send()

    all_terms_sent(0, jnp.where(top, y + 1, ny), jnp.where(top, ny, turned(2)) if ring else ny)

    @pl.when(jnp.logical_not(top))
    def _():
        ring_sent(0)

    @pl.when(odd)
    def _():
        all_terms_sent(ny, ny, turned(2) if ring else ny)
        ring_sent(1)

    def dw_sent(chip, carry):
        y_copy(chip).wait_send()

        @pl.when(chip != u)
        def _():
            w_copy(chip, u).wait_send()

        return carry

    lax.fori_loop(0, chips, dw_sent, 0)


def on_device(n, hidden, key_weight, queries, values, map_out, log_sums, out_grad, mixing, out_gain):
    rows, model = hidden.shape
    heads = mixing.shape[0]
    k_cols = key_weight.shape[1]
    q_cols = queries.shape[1]
    chips = n // 2
    ny = chips // PLANES
    width = model // n
    vm = pltpu.VMEM
    dma = pltpu.SemaphoreType.DMA
    anywhere = pl.BlockSpec(memory_space=pl.ANY)
    inside = pl.BlockSpec(memory_space=pltpu.VMEM)
    tall = vm((2 * rows, heads * rows), BF16)
    slots = vm((2 * ny, rows, k_cols), BF16)
    results = pl.pallas_call(
        functools.partial(kernel, n, heads),
        out_shape=(
            jax.ShapeDtypeStruct((rows, q_cols), BF16),
            jax.ShapeDtypeStruct((rows, k_cols), BF16),
            jax.ShapeDtypeStruct((rows, V_DIM), BF16),
            jax.ShapeDtypeStruct((width, k_cols), F32),
        ),
        in_specs=[pl.BlockSpec(memory_space=pltpu.SMEM)] + [anywhere] * 8,
        out_specs=(inside,) * 4,
        scratch_shapes=[
            vm((rows, model), BF16),
            vm((model, k_cols), BF16),
            vm((rows, 2 * heads * V_DIM), BF16),
            vm((2 * heads, rows), F32),
            vm((rows, heads * V_DIM), BF16),
            vm((1, V_DIM), F32),
            vm((2 * ny, 2 * rows, k_cols), BF16),
            vm((2 * ny, 2 * rows, V_DIM), BF16),
            vm((2 * ny, k_cols, 2 * rows), BF16),
            vm((PLANES, rows, q_cols), BF16),
            vm((PLANES, rows, heads * V_DIM), BF16),
            vm((q_cols, rows), BF16),
            vm((heads * V_DIM, rows), BF16),
            vm((PLANES, 4 * heads, rows), F32),
            vm((q_cols, rows), F32),
            vm((q_cols, rows), F32),
            vm((PLANES, q_cols, rows), BF16),
            vm((PLANES, q_cols, rows), BF16),
            tall, tall, tall,
            vm((2 * ny, 2 * rows, k_cols), F32),
            vm((2 * ny, 2 * rows, V_DIM), F32),
            slots, slots, slots, slots, slots, slots, slots, slots,
            vm((k_cols, rows), BF16),
            vm((chips, k_cols, width), BF16),
            vm((chips, k_cols, width), BF16),
            vm((chips, k_cols, width), BF16),
            vm((chips, k_cols, width), BF16),
            vm((2, rows, k_cols), BF16),
            vm((2, rows, k_cols), BF16),
            vm((rows, k_cols), F32),
            vm((rows, V_DIM), F32),
            vm((2, 2, rows, k_cols), BF16),
            dma((8,)),
            dma((2, 2 * ny)), dma((2, 2 * ny)),
            dma((2, 2 * ny)), dma((2, 2 * ny)),
            dma((3, PLANES)), dma((3, PLANES)), dma((2,)),
            dma((PLANES,)), dma((PLANES,)),
            dma((2, 2 * ny)), dma((2, 2 * ny)),
            dma((2, 2 * ny)), dma((2, 2 * ny)),
            dma((chips,)), dma((chips,)),
            dma((chips,)), dma((chips,)),
            dma((2,)), dma((2,)),
            dma((2,)), dma((2,)),
            dma((2, 2)), dma((2, 2)),
            dma((2, 2)), dma((2, 2)),
        ],
        compiler_params=pltpu.CompilerParams(
            collective_id=0, has_side_effects=True, vmem_limit_bytes=63 * 1024 * 1024),
    )(mixing, hidden, key_weight, queries, values, map_out, log_sums, out_grad, out_gain.reshape(1, -1))
    return pl.pallas_call(
        write_out,
        out_shape=tuple(jax.ShapeDtypeStruct(r.shape, r.dtype) for r in results),
        in_specs=[inside] * 4,
        out_specs=(anywhere,) * 4,
        scratch_shapes=[dma((4,))],
    )(*results)


def solution(mesh):
    placed = (
        P("sp", None),
        P(None, "tp"),
        P("sp", "tp"),
        P("sp", "tp"),
        P("sp", "tp"),
        P("tp", "sp"),
        P("sp", "tp"),
        P("tp"),
        P(),
    )
    return jax.shard_map(
        functools.partial(on_device, mesh.shape["sp"]),
        mesh=mesh,
        in_specs=placed,
        out_specs=(P("sp", "tp"), P("sp", "tp"), P("sp", "tp"), P("sp", "tp")),
        check_vma=False,
    )
```
